128 devices in a mesh: ep: 128 (over z, y, x, core).
Axes of the slice: x: 4, y: 4, z: 4, core: 2. Of those that a mesh axis runs over, the one named last changes fastest.
Arguments:
- hidden_in: bfloat16 [256, 2048], P('ep'), may hold values from -6 to 6
- lengths: int32 [256], P('ep'), may hold values from 1 to 1024, as said below
- key_cache: bfloat16 [256, 1024, 512], P('ep'), may hold values from -30 to 30
- value_cache: bfloat16 [256, 1024, 512], P('ep'), may hold values from -6 to 6
- query_w: bfloat16 [2048, 2048], P('ep'), may hold values from -0.125 to 0.125
- key_w: bfloat16 [2048, 512], P('ep'), may hold values from -0.125 to 0.125
- value_w: bfloat16 [2048, 512], P('ep'), may hold values from -0.125 to 0.125
- out_w: bfloat16 [2048, 2048], P('ep'), may hold values from -0.125 to 0.125
- lam_heads: float32 [8], replicated, may hold values from 0.3 to 0.8
- head_gain: float32 [256], replicated, may hold values from 0.1 to 1.9
- attn_gain: float32 [2048], replicated, may hold values from 0.1 to 1.9
- moe_gain: float32 [2048], replicated, may hold values from 0.1 to 1.9
- routing: int32 [256, 6], replicated, may hold values from 0 to 127, all different within a row; in each aligned block of 256 rows (0 to 255, 256 to 511, ...) at most 24 rows name the same one
- route_weight: float32 [256, 6], replicated, may hold values from 0.1 to 0.6
- gate_w: bfloat16 [128, 2048, 512], P('ep'), may hold values from -0.125 to 0.125
- up_w: bfloat16 [128, 2048, 512], P('ep'), may hold values from -0.125 to 0.125
- down_w: bfloat16 [128, 512, 2048], P('ep'), may hold values from -0.25 to 0.25
- shared_gate: bfloat16 [2048, 512], replicated, may hold values from -0.125 to 0.125
- shared_up: bfloat16 [2048, 512], replicated, may hold values from -0.125 to 0.125
- shared_down: bfloat16 [512, 2048], replicated, may hold values from -0.25 to 0.25
Outputs:
- layer_out: bfloat16 [256, 2048], P('ep')
- key_new: bfloat16 [256, 512], P('ep')
- value_new: bfloat16 [256, 512], P('ep')
The draws below stay inside these ranges and needn't reach their ends.
Inputs may be any that keep to these rules, and one draw needn't show every extreme that they name: `lengths`: some sequence has exactly 1024 positions in use. `routing`: each row names 6 different experts; no expert is named by more than 24 rows, a bound that some block reaches.
All inputs are finite; a program needn't handle non-finite values.
Results may differ from the reference program's by a relative error of at most 0.013.
The reference program's roundings to bfloat16 on the way count: a program that leaves them out, or rounds other values in their place, can miss the bound.
Values may be sent and summed in bfloat16 or wider, within the bound.
A program may use at most 64 MiB of HBM per device.

```python
import math
import jax
import jax.numpy as jnp
import numpy as np
from jax import lax

D = 2048
HEADS = 8
KV_HEADS = 2
HEAD_DIM = 128
VALUE_DIM = 256
EXPERT_DIM = 512
SHARED_DIM = 512
TOPK = 6
CACHE = 1024
SEQS = 256
EXPERTS = 128
EXP_CAP = 24


def draw_lengths(key, part):
    first_key, second_key = jax.random.split(key, 2)
    drawn = jax.random.randint(first_key, (SEQS,), 1, CACHE + 1, jnp.int32)
    chosen = jax.random.randint(second_key, (), 0, SEQS, jnp.int32)
    return jnp.where(jnp.arange(SEQS, dtype=jnp.int32) == chosen, CACHE, drawn).astype(jnp.int32)


def draw_key_cache(key, part):
    first_key = jax.random.fold_in(key, 0)
    shape = (SEQS, CACHE, KV_HEADS * 2 * HEAD_DIM)
    drawn = jnp.clip(1.75 * jax.random.normal(first_key, shape, jnp.float32), -14.0, 14.0)
    return drawn.astype(jnp.bfloat16)


def block_levels(own_key, extent, cuts, smallest, high):
    factor_of = 1.0
    for axis_at, shards_of in cuts:
        heights = jax.random.uniform(jax.random.fold_in(jax.random.fold_in(own_key, 6), axis_at), (shards_of,), jnp.float32, smallest / len(cuts), high / len(cuts))
        factor_of = factor_of * jnp.repeat(jnp.exp(heights), extent[axis_at] // shards_of).reshape((-1,) + (1,) * (len(extent) - 1 - axis_at))
    return factor_of


def deal_out(stream_key, own, number, rows, count, top, reach, slope):
    ranking = jax.random.permutation(stream_key, count)
    packed, ordinary = shares(count, rows * top, reach, slope, True), shares(count, rows * top, reach, slope, False)
    places = jnp.arange(count)

    def named(tallies, offset_by):
        used = int((tallies > 0).sum())
        fixed = max(1, used // 4)
        shifted = fixed + (places - fixed + offset_by * (used - fixed)) % max(1, count - fixed)
        return jnp.zeros((count,), jnp.int32).at[ranking[jnp.where(places < fixed, places, shifted)]].set(jnp.asarray(tallies, jnp.int32))

    tallies = jnp.where(number % 4 == 0, named(packed, number // 4), named(ordinary, number - number // 4 - 1))
    mixed = jax.random.permutation(jax.random.fold_in(own, 3), count)
    donor, receiver = mixed[0:count // 2 * 2:2], mixed[1:count // 2 * 2:2]
    margin = jnp.minimum(tallies[donor] - 1, reach - tallies[receiver]) // 2
    margin = jnp.where((donor == ranking[0]) | (receiver == ranking[0]) | (tallies[receiver] == 0), 0, jnp.maximum(margin, 0))
    shifted = jax.random.randint(jax.random.fold_in(own, 4), (count // 2,), 0, 1 << 20) % (margin + 1)
    tallies = tallies.at[donor].add(-shifted).at[receiver].add(shifted)
    items = jnp.searchsorted(jnp.cumsum(tallies), jnp.arange(rows * top), side="right").astype(jnp.int32)
    table = items.reshape(top, rows).T
    table = table[jax.random.permutation(jax.random.fold_in(own, 1), rows)]
    offset_by = jax.random.randint(jax.random.fold_in(own, 2), (rows, 1), 0, top)
    return jnp.take_along_axis(table, (jnp.arange(top)[None, :] + offset_by) % top, axis=1)


def shares(number_of, total, bound, lean, full):
    portions = [(1 << 20) // math.isqrt(grade ** lean) + 1 for grade in range(1, number_of + 1)]
    largest = bound if full else min(bound, max(-(-total // number_of), total * portions[0] // sum(portions)))
    least = 1 if total - largest >= number_of - 1 else 0
    counts, surplus = [largest] + [least] * (number_of - 1), total - largest - least * (number_of - 1)
    while surplus > 0:
        candidates = [i for i in range(1, number_of) if counts[i] < largest] or [i for i in range(1, number_of) if counts[i] < bound]
        whole, left = sum([portions[i] for i in candidates]), surplus
        for i in candidates:
            more = min(bound - counts[i], max(1, left * portions[i] // whole), surplus)
            counts[i] = counts[i] + more
            surplus = surplus - more
    return np.array(counts)


def noise(stream_key, shape, scale, most, pieces=(), kind=jnp.bfloat16):
    values = jax.random.normal(stream_key, shape, jnp.float32) * scale
    if len(pieces) > 0:
        values = block_levels(stream_key, shape, pieces, -0.22, 0.18) * values
    return jnp.clip(values, min=-most, max=most).astype(kind)


def setup_inputs(seed: int = 0) -> dict:
    key_list = jax.random.split(jax.random.key(seed), 21)
    hidden_in = noise(key_list[0], (SEQS, D), 1.0, 6.0, ((0, 128),))
    lengths = draw_lengths(jax.random.fold_in(key_list[20], 71), 0)
    key_cache = draw_key_cache(jax.random.fold_in(key_list[20], 71), 0)
    value_cache = noise(key_list[3], (SEQS, CACHE, KV_HEADS * VALUE_DIM), 1.0, 6.0, ((0, 128),))
    query_w = noise(key_list[4], (D, HEADS * 2 * HEAD_DIM), D ** -0.5, 0.125, ((0, 128),))
    key_w = noise(key_list[5], (D, KV_HEADS * 2 * HEAD_DIM), D ** -0.5, 0.125, ((0, 128),))
    value_w = noise(key_list[6], (D, KV_HEADS * VALUE_DIM), D ** -0.5, 0.125, ((0, 128),))
    out_w = noise(key_list[7], (HEADS * VALUE_DIM, D), (HEADS * VALUE_DIM) ** -0.5, 0.125, ((0, 128),))
    lam_heads = jnp.clip(jax.random.uniform(key_list[8], (HEADS,), jnp.float32, 0.3, 0.8), 0.3, 0.8)
    head_gain = jnp.clip(1.0 + 0.18 * jax.random.normal(key_list[9], (VALUE_DIM,), jnp.float32), 0.1, 1.9)
    attn_gain = jnp.clip(1.0 + 0.18 * jax.random.normal(key_list[10], (D,), jnp.float32), 0.1, 1.9)
    moe_gain = jnp.clip(1.0 + 0.18 * jax.random.normal(key_list[11], (D,), jnp.float32), 0.1, 1.9)
    routing_keys = jax.random.split(jax.random.fold_in(key_list[12], 1), SEQS // SEQS)
    routing_turns = jax.random.permutation(jax.random.fold_in(key_list[12], 3), SEQS // SEQS)
    routing = jax.vmap(lambda own, number: deal_out(jax.random.fold_in(key_list[12], 2), own, number, SEQS, EXPERTS, TOPK, EXP_CAP, 1))(routing_keys, routing_turns).reshape((SEQS, TOPK))
    route_weight = jnp.clip(jnp.exp(jax.random.uniform(key_list[13], (SEQS, TOPK), jnp.float32, math.log(0.1), math.log(0.6))), 0.1, 0.6)
    gate_w = noise(key_list[14], (EXPERTS, D, EXPERT_DIM), D ** -0.5, 0.125, ((0, 128),))
    up_w = noise(key_list[15], (EXPERTS, D, EXPERT_DIM), D ** -0.5, 0.125, ((0, 128),))
    down_w = noise(key_list[16], (EXPERTS, EXPERT_DIM, D), EXPERT_DIM ** -0.5, 0.25, ((0, 128),))
    shared_gate = noise(key_list[17], (D, SHARED_DIM), D ** -0.5, 0.125)
    shared_up = noise(key_list[18], (D, SHARED_DIM), D ** -0.5, 0.125)
    shared_down = noise(key_list[19], (SHARED_DIM, D), SHARED_DIM ** -0.5, 0.25)
    return dict(hidden_in=hidden_in, lengths=lengths, key_cache=key_cache, value_cache=value_cache, query_w=query_w, key_w=key_w, value_w=value_w, out_w=out_w, lam_heads=lam_heads, head_gain=head_gain, attn_gain=attn_gain, moe_gain=moe_gain, routing=routing, route_weight=route_weight, gate_w=gate_w, up_w=up_w, down_w=down_w, shared_gate=shared_gate, shared_up=shared_up, shared_down=shared_down)


eps_norm = 1e-06
eps_head = 1e-05
theta_base = 500000.0

def rms_scale(row_block, gain_vec, epsilon):
    row_block = row_block.astype(jnp.float32)
    return row_block * lax.rsqrt(lax.optimization_barrier(jnp.mean(row_block * row_block, axis=-1, keepdims=True)) + epsilon) * gain_vec.astype(jnp.float32)

def rotate(vectors, positions):
    half_width = vectors.shape[-1] // 2
    inverse = theta_base ** (-jnp.arange(half_width, dtype=jnp.float32) / half_width)
    angles = positions.astype(jnp.float32)[..., None] * inverse
    cosine, sine_part = (jnp.cos(angles), jnp.sin(angles))
    lower_half, upper_half = (vectors[..., :half_width], vectors[..., half_width:])
    return jnp.concatenate([lower_half * cosine - upper_half * sine_part, lower_half * sine_part + upper_half * cosine], axis=-1)

def attend(queries, key_new, value_new, cache_keys, cache_values, lengths, lam_heads, head_gain):
    num_seqs, kv_heads, group_size = (queries.shape[0], queries.shape[1], queries.shape[2])
    head_dim = queries.shape[-1]
    cache_len = cache_keys.shape[1]
    cache_keys = cache_keys.reshape(num_seqs, cache_len, kv_heads, 2, head_dim).astype(jnp.float32)
    cache_values = cache_values.reshape(num_seqs, cache_len, kv_heads, -1).astype(jnp.float32)
    value_new = value_new.reshape(num_seqs, kv_heads, -1)
    queries = queries.astype(jnp.float32)
    score_scale = head_dim ** (-0.5)
    scores = jnp.einsum('skgph,sckph->skgpc', queries, cache_keys) * score_scale
    self_score = jnp.einsum('skgph,skph->skgp', queries, key_new.astype(jnp.float32)) * score_scale
    live_mask = (jnp.arange(cache_len)[None, :] < lengths[:, None])[:, None, None, None, :]
    peak = jnp.maximum(lax.optimization_barrier(jnp.max(jnp.where(live_mask, scores, -jnp.inf), axis=-1)), self_score)
    weights = jnp.where(live_mask, jnp.exp(scores - peak[..., None]), 0.0)
    self_weight = jnp.exp(self_score - peak)
    totals = lax.optimization_barrier(jnp.sum(weights, axis=-1)) + self_weight
    lambda_grid = lam_heads.reshape(kv_heads, group_size)[None]
    combined = (weights[:, :, :, 0] / totals[:, :, :, 0, None] - lambda_grid[..., None] * weights[:, :, :, 1] / totals[:, :, :, 1, None]).astype(jnp.bfloat16)
    self_combined = (self_weight[..., 0] / totals[..., 0] - lambda_grid * self_weight[..., 1] / totals[..., 1]).astype(jnp.bfloat16)
    head_out = jnp.einsum('skgc,sckv->skgv', combined.astype(jnp.float32), cache_values)
    head_out = head_out + self_combined.astype(jnp.float32)[..., None] * value_new.astype(jnp.float32)[:, :, None, :]
    return rms_scale(head_out, head_gain, eps_head).astype(jnp.bfloat16).reshape(num_seqs, -1)

def routed_sum(moe_in, routing, route_weight, gate_w, up_w, down_w):

    def add_expert(running, expert_id):
        routed_here = lax.optimization_barrier(jnp.sum((routing == expert_id).astype(jnp.int32), axis=1))
        weight_col = lax.optimization_barrier(jnp.sum(jnp.where(routing == expert_id, route_weight, 0.0), axis=1))
        slot_index = jnp.cumsum(routed_here) - 1
        pick_table = ((slot_index[None, :] == jnp.arange(EXP_CAP)[:, None]) & (routed_here[None, :] > 0)).astype(jnp.float32)
        picked = jnp.dot(pick_table, moe_in.astype(jnp.float32)).astype(jnp.bfloat16)
        gate_one = lax.dynamic_index_in_dim(gate_w, expert_id, 0, keepdims=False)
        up_one = lax.dynamic_index_in_dim(up_w, expert_id, 0, keepdims=False)
        down_one = lax.dynamic_index_in_dim(down_w, expert_id, 0, keepdims=False)
        hidden = (jax.nn.silu(jnp.dot(picked, gate_one, preferred_element_type=jnp.float32)) * jnp.dot(picked, up_one, preferred_element_type=jnp.float32)).astype(jnp.bfloat16)
        result = jnp.dot(hidden, down_one, preferred_element_type=jnp.float32).astype(jnp.bfloat16)
        return (running + jnp.dot(pick_table.T, result.astype(jnp.float32)) * weight_col[:, None], None)
    start_sum = jnp.zeros(moe_in.shape, jnp.float32)
    running, unused = lax.scan(add_expert, start_sum, jnp.arange(gate_w.shape[0], dtype=jnp.int32))
    return running

def reference(hidden_in, lengths, key_cache, value_cache, query_w, key_w, value_w, out_w, lam_heads, head_gain, attn_gain, moe_gain, routing, route_weight, gate_w, up_w, down_w, shared_gate, shared_up, shared_down):
    num_seqs = hidden_in.shape[0]
    normed = rms_scale(hidden_in, attn_gain, eps_norm).astype(jnp.bfloat16)
    q_raw = jnp.dot(normed, query_w, preferred_element_type=jnp.float32)
    k_raw = jnp.dot(normed, key_w, preferred_element_type=jnp.float32)
    value_new = jnp.dot(normed, value_w, preferred_element_type=jnp.float32).astype(jnp.bfloat16)
    queries = rotate(q_raw.reshape(num_seqs, KV_HEADS, -1, 2, HEAD_DIM), lengths[:, None, None, None]).astype(jnp.bfloat16)
    key_new = rotate(k_raw.reshape(num_seqs, KV_HEADS, 2, HEAD_DIM), lengths[:, None, None]).astype(jnp.bfloat16)

    def one_sequence(items):
        return attend(*[item[None] for item in items], lam_heads, head_gain)[0]
    attn_out = lax.map(one_sequence, (queries, key_new, value_new, key_cache, value_cache, lengths))
    attn_proj = jnp.dot(attn_out, out_w, preferred_element_type=jnp.float32).astype(jnp.bfloat16)
    after_mixer = (hidden_in.astype(jnp.float32) + attn_proj.astype(jnp.float32)).astype(jnp.bfloat16)
    moe_in = rms_scale(after_mixer, moe_gain, eps_norm).astype(jnp.bfloat16)
    routed = routed_sum(moe_in, routing, route_weight, gate_w, up_w, down_w)
    shared_hidden = (jax.nn.silu(jnp.dot(moe_in, shared_gate, preferred_element_type=jnp.float32)) * jnp.dot(moe_in, shared_up, preferred_element_type=jnp.float32)).astype(jnp.bfloat16)
    shared_out = jnp.dot(shared_hidden, shared_down, preferred_element_type=jnp.float32)
    layer_out = (after_mixer.astype(jnp.float32) + routed + shared_out).astype(jnp.bfloat16)
    return (layer_out, key_new.reshape(num_seqs, -1), value_new)
```

```python
import jax
import jax.numpy as jnp
from jax import lax
from jax.experimental import pallas as pl
from jax.experimental.pallas import tpu as pltpu
from jax.sharding import PartitionSpec as P

F32 = jnp.float32
BF16 = jnp.bfloat16
MESH = pl.DeviceIdType.MESH
ANY = pl.ANY
N = 128
D = 2048
CACHE = 1024
SLOTS = 32
W, O, HID, P1, P2, P3, P4, P5, P6, P7 = range(10)


def dot(a, b):
    return jnp.dot(a, b, preferred_element_type=F32)


def rms(x, gain, eps):
    return x * lax.rsqrt(jnp.mean(x * x, axis=-1, keepdims=True) + eps) * gain


def kernel(
    lengths, hidden, cosine, sine, lam, hgain, again, mgain, routing, rweight,
    qw, kw, vw, ow, kc_h, vc_h, gate_h, up_h, down_h, sg_h, su_h, sd_h,
    out, key_out, val_out,
    wcat, obuf_s, wbuf, obuf, kc, vc, gate, up, down, sg, su, sd,
    hs, hbuf, s1, r1, lhs, part, s2, r2, qscr, kscr, vscr, s3, r3, r4, am, gat, res, racc, s7, r7,
    loc, snd, rcv,
):
    me = lax.axis_index("ep")
    z = me // 32
    plane = me % 32
    y = plane // 8
    xc = me % 8
    row = me // 8
    slab = z * 8 + xc

    def local(src, dst, i):
        return pltpu.make_async_copy(src, dst, loc.at[i])

    locals_ = [
        local(qw, wcat.at[:, pl.ds(0, 2048)], 0),
        local(kw, wcat.at[:, pl.ds(2048, 512)], 1),
        local(vw, wcat.at[:, pl.ds(2560, 512)], 2),
        local(ow, obuf_s, 3),
        local(kc_h, kc, 4),
        local(vc_h, vc, 5),
        local(gate_h.at[0], gate, 6),
        local(up_h.at[0], up, 7),
        local(down_h.at[0], down, 8),
        local(sg_h, sg, 9),
        local(su_h, su, 10),
        local(sd_h.at[:, pl.ds(pl.multiple_of(xc * 256, 256), 256)], sd, 11),
    ]
    for c in locals_:
        c.start()

    barrier = pltpu.get_barrier_semaphore()

    def greet(r, carry):
        pl.semaphore_signal(barrier, inc=1, device_id=((me + r) % N,), device_id_type=MESH)
        return carry

    lax.fori_loop(1, N, greet, 0)

    def remote(src, dst, phase, device):
        return pltpu.make_async_remote_copy(
            src_ref=src, dst_ref=dst, send_sem=snd.at[phase], recv_sem=rcv.at[phase],
            device_id=(device,), device_id_type=MESH,
        )

    def arrived(ref, phase):
        remote(ref, ref, phase, (me + 1) % N).wait_recv()

    def left(ref, phase):
        remote(ref, ref, phase, (me + 1) % N).wait_send()

    h32 = hidden[...].astype(F32)
    normed = rms(h32, again[...], 1e-6).astype(BF16).astype(F32)
    for yy in range(4):
        for zz in range(4):
            s1[yy, :, zz * 128 : zz * 128 + 128] = normed[:, zz * 512 + yy * 128 : zz * 512 + yy * 128 + 128]
    for j in range(8):
        hs[j] = h32[:, j * 256 : j * 256 + 256]

    for c in locals_[:4]:
        c.wait()
    pl.semaphore_wait(barrier, N - 1)

    def send_w(r, carry):
        t = (slab + r) % 32
        col = pl.multiple_of((t % 8) * 384, 128)
        at = pl.multiple_of(slab * 16, 16)
        device = (t // 8) * 32 + y * 8 + t % 8
        remote(wcat.at[:, pl.ds(col, 384)], wbuf.at[pl.ds(at, 16), :], W, device).start()
        return carry

    def send_1(r, carry):
        t = (plane + r) % 32
        remote(s1.at[t // 8], r1.at[plane], P1, z * 32 + t).start()
        return carry

    def send_h(r, carry):
        t = (xc + r) % 8
        remote(hs.at[t], hbuf.at[xc], HID, row * 8 + t).start()
        return carry

    def send_o(r, carry):
        t = (slab + r) % 32
        col = pl.multiple_of((t % 8) * 256, 128)
        at = pl.multiple_of(slab * 16, 16)
        device = (t // 8) * 32 + y * 8 + t % 8
        remote(obuf_s.at[:, pl.ds(col, 256)], obuf.at[pl.ds(at, 16), :], O, device).start()
        return carry

    lax.fori_loop(1, 32, send_1, 0)
    lax.fori_loop(1, 32, send_w, 0)
    lax.fori_loop(1, 8, send_h, 0)
    lax.fori_loop(1, 32, send_o, 0)

    own = pl.ds(pl.multiple_of(slab * 16, 16), 16)
    wbuf[own, :] = wcat[:, pl.ds(pl.multiple_of(xc * 384, 128), 384)]
    obuf[own, :] = obuf_s[:, pl.ds(pl.multiple_of(xc * 256, 128), 256)]
    r1[plane] = s1[y]
    hbuf[xc] = hs[xc]

    routed = routing[...] == me
    wcol = jnp.sum(jnp.where(routed, rweight[...], 0.0), axis=1, keepdims=True)
    here = jnp.sum(jnp.where(routed, 1.0, 0.0), axis=1, keepdims=True)
    here = jnp.broadcast_to(here, (256, 128))
    before = lax.broadcasted_iota(jnp.int32, (256, 256), 1) < lax.broadcasted_iota(jnp.int32, (256, 256), 0)
    rank = dot(jnp.where(before, 1.0, 0.0).astype(BF16), here.astype(BF16))
    slot = lax.broadcasted_iota(jnp.int32, (256, 128), 1).astype(F32)
    back = jnp.where(rank == slot, here, 0.0)
    pick = back.T[:SLOTS].astype(BF16)
    back = back.astype(BF16)

    arrived(r1.at[pl.ds(0, 31)], P1)
    for i in range(32):
        lhs[2 * i : 2 * i + 2, :] = r1[i]
    arrived(wbuf.at[pl.ds(0, 496), :], W)
    part[...] = dot(lhs[...].astype(BF16), wbuf[...])
    for i in range(32):
        s2[i] = part[2 * i : 2 * i + 2, :]

    def send_2(r, carry):
        t = (plane + r) % 32
        remote(s2.at[t], r2.at[plane], P2, z * 32 + t).start()
        return carry

    lax.fori_loop(1, 32, send_2, 0)
    r2[plane] = s2[plane]
    arrived(r2.at[pl.ds(0, 31)], P2)

    for u in range(24):
        cb, at = u // 3, (u % 3) * 128
        val = r2[cb, :, at : at + 128]
        for yy in range(1, 4):
            val = val + r2[yy * 8 + cb, :, at : at + 128]
        for s in range(2):
            line = val[s : s + 1, :]
            if u < 16:
                r = (u % 2) * 8 + u // 2
                qscr[s, r : r + 1, :] = line
            elif u < 20:
                kscr[s, u - 16 : u - 15, :] = line
            else:
                v = u - 20
                vscr[s, v // 2 : v // 2 + 1, (v % 2) * 128 : (v % 2) * 128 + 128] = line

    for c in locals_[4:6]:
        c.wait()
    rows = lax.broadcasted_iota(jnp.int32, (16, 1), 0)
    pair_of = (rows // 8) + 2 * ((rows % 8) // 4)
    head = lax.broadcasted_iota(jnp.int32, (8, 1), 0)
    diag = lax.broadcasted_iota(jnp.int32, (8, 8), 0) == lax.broadcasted_iota(jnp.int32, (8, 8), 1)
    lam_col = jnp.sum(jnp.where(diag, lam[...], 0.0), axis=1, keepdims=True)
    scale = 128 ** (-0.5)
    place = lax.broadcasted_iota(jnp.int32, (1, CACHE), 1)
    for s in range(2):
        cos_row, sin_row = cosine[s : s + 1, :], sine[s : s + 1, :]

        def turn(v):
            return (v * cos_row + pltpu.roll(v, 64, 1) * sin_row).astype(BF16)

        q = turn(qscr[s]).astype(F32)
        kn = turn(kscr[s])
        vn = vscr[s].astype(BF16)
        for u in range(4):
            key_out[s : s + 1, u * 128 : u * 128 + 128] = kn[u : u + 1]
        for u in range(2):
            val_out[s : s + 1, u * 256 : u * 256 + 256] = vn[u : u + 1]
        kn = kn.astype(F32)
        vn = vn.astype(F32)
        wide = jnp.concatenate([jnp.where(pair_of == u, q, 0.0) for u in range(4)], axis=1).astype(BF16)
        scores = lax.dot_general(wide, kc[s], (((1,), (1,)), ((), ())), preferred_element_type=F32) * scale
        k_of = jnp.where(
            pair_of == 0, kn[0:1], jnp.where(pair_of == 1, kn[1:2], jnp.where(pair_of == 2, kn[2:3], kn[3:4]))
        )
        own_score = jnp.sum(q * k_of, axis=1, keepdims=True) * scale
        live = place < lengths[s]
        peak = jnp.maximum(jnp.max(jnp.where(live, scores, -jnp.inf), axis=1, keepdims=True), own_score)
        weights = jnp.where(live, jnp.exp(scores - peak), 0.0)
        own_weight = jnp.exp(own_score - peak)
        totals = jnp.sum(weights, axis=1, keepdims=True) + own_weight
        maps = weights / totals
        own_maps = own_weight / totals
        combined = (maps[:8] - lam_col * maps[8:]).astype(BF16)
        own_comb = (own_maps[:8] - lam_col * own_maps[8:]).astype(BF16).astype(F32)
        both = dot(combined, vc[s])
        first = head < 4
        head_out = jnp.where(first, both[:, :256], both[:, 256:])
        head_out = head_out + own_comb * jnp.where(first, vn[0:1], vn[1:2])
        att = rms(head_out, hgain[...], 1e-5).astype(BF16).astype(F32)
        for yy in range(4):
            for zz in range(4):
                h, half = (4 * zz + yy) // 2, yy % 2
                s3[yy, s : s + 1, zz * 128 : zz * 128 + 128] = att[h : h + 1, half * 128 : half * 128 + 128]

    def send_3(r, carry):
        t = (plane + r) % 32
        remote(s3.at[t // 8], r3.at[plane], P3, z * 32 + t).start()
        return carry

    lax.fori_loop(1, 32, send_3, 0)
    r3[plane] = s3[y]
    arrived(obuf.at[pl.ds(0, 496), :], O)
    arrived(hbuf.at[pl.ds(0, 7)], HID)
    arrived(r3.at[pl.ds(0, 31)], P3)
    left(r1.at[pl.ds(0, 31)], P1)
    for i in range(32):
        lhs[2 * i : 2 * i + 2, :] = r3[i]
    proj = dot(lhs[...].astype(BF16), obuf[...])
    s2b = part
    s2b[:, :256] = proj

    def send_4(r, carry):
        t = (y + r) % 4
        remote(
            s2b.at[pl.ds(pl.multiple_of(t * 16, 16), 16), pl.ds(0, 256)], r4.at[y], P4, z * 32 + t * 8 + xc
        ).start()
        return carry

    lax.fori_loop(1, 4, send_4, 0)
    r4[y] = s2b[pl.ds(pl.multiple_of(y * 16, 16), 16), pl.ds(0, 256)]
    for i in range(8):
        lhs[2 * i : 2 * i + 2, 0:256] = hbuf[i]
    arrived(r4.at[pl.ds(0, 3)], P4)
    proj = (r4[0] + r4[1]) + (r4[2] + r4[3])
    mixed = (lhs[0:16, 0:256] + proj.astype(BF16).astype(F32)).astype(BF16)
    am[...] = mixed
    gat[xc, row] = mixed

    def send_5(r, carry):
        remote(am, gat.at[xc, row], P5, (me + r) % N).start()
        return carry

    lax.fori_loop(1, N, send_5, 0)
    for c in locals_[6:]:
        c.wait()
    arrived(racc.at[pl.ds(0, N - 1)], P5)

    def normed_rows(blocks):
        total = jnp.sum(blocks[0] * blocks[0], axis=1, keepdims=True)
        for b in blocks[1:]:
            total = total + jnp.sum(b * b, axis=1, keepdims=True)
        factor = lax.rsqrt(total / D + 1e-6)
        return jnp.concatenate(
            [(b * factor * mgain[:, i * 256 : i * 256 + 256]).astype(BF16) for i, b in enumerate(blocks)], axis=1
        )

    moe = normed_rows([dot(pick, gat[b].reshape(256, 256)) for b in range(8)])
    hid = (jax.nn.silu(dot(moe, gate[...])) * dot(moe, up[...])).astype(BF16)
    answer = dot(hid, down[...]).astype(BF16)
    answer = jnp.concatenate([answer, jnp.zeros((128 - SLOTS, D), BF16)], axis=0)
    for b in range(8):
        spread = dot(back, answer[:, b * 256 : b * 256 + 256]) * wcol
        res[b] = spread.astype(BF16).reshape(16, 16, 256)

    def send_6(r, carry):
        t = (me + r) % N
        remote(res.at[t % 8, t // 8], racc.at[me], P6, t).start()
        return carry

    lax.fori_loop(1, N, send_6, 0)
    racc[me] = res[xc, row]

    moe = normed_rows([gat[b, row].astype(F32) for b in range(8)])
    hid = (jax.nn.silu(dot(moe, sg[...])) * dot(moe, su[...])).astype(BF16)
    total = dot(hid, sd[...])
    arrived(racc.at[pl.ds(0, N - 1)], P6)

    def add(i, carry):
        return carry + racc[i].astype(F32)

    total = am[...].astype(F32) + (lax.fori_loop(0, N, add, jnp.zeros((16, 256), F32)) + total)
    total = total.astype(BF16).astype(F32)
    for i in range(8):
        s7[i] = total[2 * i : 2 * i + 2, :]

    def send_7(r, carry):
        t = (xc + r) % 8
        remote(s7.at[t], r7.at[xc], P7, row * 8 + t).start()
        return carry

    lax.fori_loop(1, 8, send_7, 0)
    r7[xc] = s7[xc]
    left(wbuf.at[pl.ds(0, 496), :], W)
    left(obuf.at[pl.ds(0, 496), :], O)
    left(hbuf.at[pl.ds(0, 7)], HID)
    left(r2.at[pl.ds(0, 31)], P2)
    left(r3.at[pl.ds(0, 31)], P3)
    left(r4.at[pl.ds(0, 3)], P4)
    left(racc.at[pl.ds(0, N - 1)], P5)
    left(racc.at[pl.ds(0, N - 1)], P6)
    arrived(r7.at[pl.ds(0, 7)], P7)
    for j in range(8):
        out[:, j * 256 : j * 256 + 256] = r7[j].astype(BF16)
    left(r7.at[pl.ds(0, 7)], P7)


def on_device(
    hidden_in, lengths, key_cache, value_cache, query_w, key_w, value_w, out_w, lam_heads, head_gain,
    attn_gain, moe_gain, routing, route_weight, gate_w, up_w, down_w, shared_gate, shared_up, shared_down,
):
    inverse = 500000.0 ** (-jnp.arange(64, dtype=F32) / 64)
    angles = lengths.astype(F32)[:, None] * inverse
    cosine, sine = jnp.cos(angles), jnp.sin(angles)
    cosine = jnp.concatenate([cosine, cosine], axis=1)
    sine = jnp.concatenate([-sine, sine], axis=1)
    vm = pl.BlockSpec(memory_space=pltpu.VMEM)
    hbm = pl.BlockSpec(memory_space=ANY)
    scratch = [
        ((16, 3072), BF16), ((16, 2048), BF16), ((512, 384), BF16), ((512, 256), BF16),
        ((2, CACHE, 512), BF16), ((2, CACHE, 512), BF16),
        ((D, 512), BF16), ((D, 512), BF16), ((512, D), BF16),
        ((D, 512), BF16), ((D, 512), BF16), ((512, 256), BF16),
        ((8, 2, 256), F32), ((8, 2, 256), F32), ((4, 2, 512), F32), ((32, 2, 512), F32),
        ((64, 512), F32), ((64, 384), F32), ((32, 2, 384), F32), ((32, 2, 384), F32),
        ((2, 16, 128), F32), ((2, 4, 128), F32), ((2, 2, 256), F32),
        ((4, 2, 512), F32), ((32, 2, 512), F32), ((4, 16, 256), F32), ((16, 256), BF16),
        ((8, 16, 16, 256), BF16), ((8, 16, 16, 256), BF16), ((N, 16, 256), BF16),
        ((8, 2, 256), F32), ((8, 2, 256), F32),
    ]
    return pl.pallas_call(
        kernel,
        out_shape=(
            jax.ShapeDtypeStruct((2, D), BF16),
            jax.ShapeDtypeStruct((2, 512), BF16),
            jax.ShapeDtypeStruct((2, 512), BF16),
        ),
        in_specs=[pl.BlockSpec(memory_space=pltpu.SMEM)] + [vm] * 9 + [hbm] * 12,
        out_specs=(vm, vm, vm),
        scratch_shapes=[pltpu.VMEM(*s) for s in scratch]
        + [pltpu.SemaphoreType.DMA((12,)), pltpu.SemaphoreType.DMA((10,)), pltpu.SemaphoreType.DMA((10,))],
        compiler_params=pltpu.CompilerParams(
            collective_id=0, has_side_effects=True, vmem_limit_bytes=60 * 1024 * 1024
        ),
    )(
        lengths, hidden_in, cosine, sine, lam_heads.reshape(1, 8), head_gain.reshape(1, 256),
        attn_gain.reshape(1, D), moe_gain.reshape(1, D), routing, route_weight,
        query_w, key_w, value_w, out_w, key_cache, value_cache, gate_w, up_w, down_w,
        shared_gate, shared_up, shared_down,
    )


def solution(mesh):
    e2, e3 = P("ep", None), P("ep", None, None)
    return jax.shard_map(
        on_device,
        mesh=mesh,
        in_specs=(
            e2, P("ep"), e3, e3, e2, e2, e2, e2, P(), P(), P(), P(), P(), P(), e3, e3, e3, P(), P(), P(),
        ),
        out_specs=(e2, e2, e2),
        check_vma=False,
    )
```

```python
import jax
import jax.numpy as jnp
from jax import lax
from jax.experimental import pallas as pl
from jax.experimental.pallas import tpu as pltpu
from jax.sharding import PartitionSpec as P

F32 = jnp.float32
BF16 = jnp.bfloat16
MESH = pl.DeviceIdType.MESH
N = 128
CHIPS = 64
D = 2048
CACHE = 1024
SLOTS = 32
OWN = 24
W, O, OX, HID, P1, P2, P3, P5, PX, AX, P6 = range(11)


def dot(a, b):
    return jnp.dot(a, b, preferred_element_type=F32)


def dot_nt(a, b):
    return lax.dot_general(a, b, (((1,), (1,)), ((), ())), preferred_element_type=F32)


def iota(shape, dim):
    return lax.broadcasted_iota(jnp.int32, shape, dim)


def rms(x, gain, eps):
    return x * lax.rsqrt(jnp.mean(x * x, axis=-1, keepdims=True) + eps) * gain


def kernel(
    lengths_h, hidden_h, lam_h, hgain_h, again_h, mgain_h, routing_h, rweight_h,
    qw, kw, vw, ow, kc_h, vc_h, gate_h, up_h, down_h, sg_h, su_h, sd_h,
    out,
    lengths, hidden, lam, hgain, again, mgain, routing, rweight,
    wcat, obuf_s, wbuf, obuf, kc, vc, gate, up, down, sg, su, sd,
    hs, hbuf, hb, s1, r1, lhs, part, s2, r2, qscr, kscr, vscr, at16, s3, r3, x3,
    am, gat, pt8, spread, mine, theirs, picked, ans, ans_x, res, racc, fin,
    loc, snd, rcv,
):
    me = lax.axis_index("ep")
    z = me // 32
    plane = me % 32
    y = plane // 8
    xc = me % 8
    c = me % 2
    chip = me // 2
    q = chip % 16
    slab = z * 8 + xc
    mate = me + 1 - 2 * c

    barrier = pltpu.get_barrier_semaphore()

    def greet(device):
        pl.semaphore_signal(barrier, inc=1, device_id=(device,), device_id_type=MESH)

    def greet_same(r, carry):
        greet((chip + r) % CHIPS * 2 + c)
        return carry

    def greet_plane(r, carry):
        greet(z * 32 + r * 2 + 1 - c)
        return carry

    def greet_slab(r, carry):
        greet((z + r // 4) % 4 * 32 + y * 8 + (r % 4) * 2 + 1 - c)
        return carry

    lax.fori_loop(1, CHIPS, greet_same, 0)
    lax.fori_loop(0, 16, greet_plane, 0)
    lax.fori_loop(4, 16, greet_slab, 0)

    pairs = [
        (hidden_h, hidden), (again_h, again),
        (qw, wcat.at[:, pl.ds(0, 2048)]), (kw, wcat.at[:, pl.ds(2048, 512)]), (vw, wcat.at[:, pl.ds(2560, 512)]),
        (routing_h, routing), (rweight_h, rweight), (ow, obuf_s),
        (kc_h, kc), (vc_h, vc), (lengths_h, lengths), (lam_h, lam), (hgain_h, hgain), (mgain_h, mgain),
        (gate_h.at[0], gate), (up_h.at[0], up), (down_h.at[0], down), (sg_h, sg), (su_h, su), (sd_h, sd),
    ]
    copies = [pltpu.make_async_copy(src, dst, loc.at[i]) for i, (src, dst) in enumerate(pairs)]
    for copy in copies:
        copy.start()

    def ready(lo, hi):
        for copy in copies[lo:hi]:
            copy.wait()

    def remote(src, dst, phase, device):
        return pltpu.make_async_remote_copy(
            src_ref=src, dst_ref=dst, send_sem=snd.at[phase], recv_sem=rcv.at[phase],
            device_id=(device,), device_id_type=MESH,
        )

    def arrived(ref, phase):
        remote(ref, ref, phase, mate).wait_recv()

    def left(ref, phase):
        remote(ref, ref, phase, mate).wait_send()

    ready(0, 2)
    h32 = hidden[...].astype(F32)
    normed = rms(h32, again[...], 1e-6).astype(BF16).astype(F32)
    for yy in range(4):
        for zz in range(4):
            s1[yy, :, zz * 128 : zz * 128 + 128] = normed[:, zz * 512 + yy * 128 : zz * 512 + yy * 128 + 128]
    for j in range(16):
        hs[j] = h32[:, j * 128 : j * 128 + 128]
    ready(2, 5)
    pl.semaphore_wait(barrier, 91)

    def send_1(r, carry):
        t = (plane + r) % 32
        remote(s1.at[t // 8], r1.at[plane], P1, z * 32 + t).start()
        return carry

    def send_w(r, carry):
        t = (slab + r) % 32
        col = pl.multiple_of((t % 8) * 384, 128)
        at = pl.multiple_of(slab * 16, 16)
        remote(wcat.at[:, pl.ds(col, 384)], wbuf.at[pl.ds(at, 16), :], W, (t // 8) * 32 + y * 8 + t % 8).start()
        return carry

    def send_h(r, carry):
        t = (q + r) % 16
        remote(hs.at[t], hbuf.at[q], HID, z * 32 + t * 2 + c).start()
        return carry

    def send_o(r, carry):
        t = (chip + r) % CHIPS
        col = pl.multiple_of((t % 16) * 128, 128)
        remote(obuf_s.at[:, pl.ds(col, 128)], obuf.at[chip, c], O, t * 2 + c).start()
        return carry

    lax.fori_loop(1, 32, send_w, 0)
    lax.fori_loop(1, 32, send_1, 0)
    own = pl.ds(pl.multiple_of(slab * 16, 16), 16)
    wbuf[own, :] = wcat[:, pl.ds(pl.multiple_of(xc * 384, 128), 384)]
    r1[plane] = s1[y]
    hbuf[q] = hs[q]

    ready(5, 8)
    obuf[chip, c] = obuf_s[:, pl.ds(pl.multiple_of(q * 128, 128), 128)]
    sel = jnp.where(
        iota((128, 256), 1) == 4 * (iota((128, 256), 0) // 2) + 2 * c + iota((128, 256), 0) % 2, 1.0, 0.0
    ).astype(BF16)
    before = jnp.where(iota((256, 256), 0) < iota((256, 256), 1), 1.0, 0.0).astype(BF16)
    picks = []
    for i, expert in enumerate((me, mate)):
        hit = routing[...] == expert
        here = jnp.sum(jnp.where(hit, 1.0, 0.0), axis=0, keepdims=True)
        rank = dot(jnp.broadcast_to(here, (16, 256)).astype(BF16), before)[0:1]
        full = jnp.where(rank == (iota((256, 256), 0) % SLOTS).astype(F32), here, 0.0)
        pt8[i] = dot_nt(sel, full.astype(BF16))
        full = full[:SLOTS]
        if i == 0:
            weight = jnp.sum(jnp.where(hit, rweight[...], 0.0), axis=0, keepdims=True)
            weight = jnp.sum(full * weight, axis=1, keepdims=True)
        mark = (iota((SLOTS, 256), 0) - OWN == iota((SLOTS, 256), 1) - 2 * expert) & (
            iota((SLOTS, 256), 1) // 2 == expert
        )
        full = full + jnp.where(mark, 1.0, 0.0)
        picks.append(dot_nt(full.astype(BF16), sel))
    picks = jnp.concatenate(picks, axis=0).astype(BF16)
    block = (iota((16, 256), 1) // SLOTS) == (iota((16, 256), 0) % 8)
    first_token = iota((16, 256), 0) < 8

    def lay(g, carry):
        for i in range(2):
            eight = pt8[i, pl.ds(pl.multiple_of(8 * g, 8), 8), :]
            for o in range(4):
                tile = jnp.where(first_token, eight[2 * o : 2 * o + 1], eight[2 * o + 1 : 2 * o + 2])
                spread[i, 4 * g + o] = jnp.where(block, tile, 0.0).astype(BF16)
        return carry

    arrived(r1.at[pl.ds(0, 31)], P1)
    for i in range(32):
        lhs[2 * i : 2 * i + 2, :] = r1[i]
    arrived(wbuf.at[pl.ds(0, 496), :], W)
    part[...] = dot(lhs[...].astype(BF16), wbuf[...])
    for i in range(32):
        s2[i] = part[2 * i : 2 * i + 2, :]

    def send_2(r, carry):
        t = (plane + r) % 32
        remote(s2.at[t], r2.at[plane], P2, z * 32 + t).start()
        return carry

    lax.fori_loop(1, 32, send_2, 0)
    r2[plane] = s2[plane]
    lax.fori_loop(1, CHIPS, send_o, 0)
    lax.fori_loop(1, 16, send_h, 0)
    lax.fori_loop(0, CHIPS // 4, lay, 0)
    arrived(r2.at[pl.ds(0, 31)], P2)

    for u in range(24):
        cb, at = u // 3, (u % 3) * 128
        val = r2[cb, :, at : at + 128]
        for yy in range(1, 4):
            val = val + r2[yy * 8 + cb, :, at : at + 128]
        for s in range(2):
            line = val[s : s + 1, :]
            if u < 16:
                r = (u % 2) * 8 + u // 2
                qscr[s, r : r + 1, :] = line
            elif u < 20:
                kscr[s, u - 16 : u - 15, :] = line
            else:
                v = u - 20
                vscr[s, v // 2 : v // 2 + 1, (v % 2) * 128 : (v % 2) * 128 + 128] = line

    ready(8, 14)
    rows = iota((16, 1), 0)
    pair_of = (rows // 8) + 2 * ((rows % 8) // 4)
    first = iota((8, 1), 0) < 4
    lam_col = jnp.sum(jnp.where(iota((8, 8), 0) == iota((8, 8), 1), lam[...], 0.0), axis=1, keepdims=True)
    scale = 128 ** (-0.5)
    place = iota((1, CACHE), 1)
    lane = iota((1, 128), 1)
    inverse = jnp.exp((lane % 64).astype(F32) * (-13.122363377404328 / 64))
    for s in range(2):
        angle = lengths[s].astype(F32) * inverse
        cos_row = jnp.cos(angle)
        sin_row = jnp.where(lane < 64, -jnp.sin(angle), jnp.sin(angle))

        def turn(v):
            return (v * cos_row + pltpu.roll(v, 64, 1) * sin_row).astype(BF16)

        qq = turn(qscr[s]).astype(F32)
        kn = turn(kscr[s])
        vn = vscr[s].astype(BF16)
        for u in range(4):
            out[s : s + 1, D + u * 128 : D + u * 128 + 128] = kn[u : u + 1]
        for u in range(2):
            out[s : s + 1, D + 512 + u * 256 : D + 512 + u * 256 + 256] = vn[u : u + 1]
        kn = kn.astype(F32)
        vn = vn.astype(F32)
        wide = jnp.concatenate([jnp.where(pair_of == u, qq, 0.0) for u in range(4)], axis=1).astype(BF16)
        scores = dot_nt(wide, kc[s]) * scale
        k_of = jnp.where(
            pair_of == 0, kn[0:1], jnp.where(pair_of == 1, kn[1:2], jnp.where(pair_of == 2, kn[2:3], kn[3:4]))
        )
        own_score = jnp.sum(qq * k_of, axis=1, keepdims=True) * scale
        live = place < lengths[s]
        peak = jnp.maximum(jnp.max(jnp.where(live, scores, -jnp.inf), axis=1, keepdims=True), own_score)
        weights = jnp.where(live, jnp.exp(scores - peak), 0.0)
        own_weight = jnp.exp(own_score - peak)
        totals = jnp.sum(weights, axis=1, keepdims=True) + own_weight
        maps = weights / totals
        own_maps = own_weight / totals
        combined = (maps[:8] - lam_col * maps[8:]).astype(BF16)
        own_comb = (own_maps[:8] - lam_col * own_maps[8:]).astype(BF16).astype(F32)
        both = dot(combined, vc[s])
        head_out = jnp.where(first, both[:, :256], both[:, 256:])
        head_out = head_out + own_comb * jnp.where(first, vn[0:1], vn[1:2])
        att = rms(head_out, hgain[...], 1e-5)
        for h in range(8):
            for half in range(2):
                at16[s, 2 * h + half : 2 * h + half + 1, :] = att[h : h + 1, half * 128 : half * 128 + 128]
        s3[s] = at16[s].astype(BF16)

    def send_3(r, carry):
        t = (q + r) % 16
        remote(s3, r3.at[q], P3, z * 32 + t * 2 + c).start()
        return carry

    lax.fori_loop(1, 16, send_3, 0)
    r3[q] = s3[...]
    arrived(obuf.at[pl.ds(0, 63), 0], O)
    remote(obuf.at[:, c], obuf.at[:, c], OX, mate).start()
    arrived(hbuf.at[pl.ds(0, 15)], HID)
    for i in range(16):
        hb[2 * i : 2 * i + 2, :] = hbuf[i]
    arrived(obuf.at[:, 0], OX)
    arrived(r3.at[pl.ds(0, 15)], P3)
    x3[...] = r3[...].reshape(512, 128).astype(F32)
    wide = jnp.concatenate([x3[pl.ds(b, 32, stride=16), :].astype(BF16) for b in range(16)], axis=1)
    proj = dot(wide, obuf[...].reshape(D, 128))
    mixed = (hb[...] + proj.astype(BF16).astype(F32)).astype(BF16)
    am[...] = mixed
    gat[q, z] = mixed

    def send_5(r, carry):
        remote(am, gat.at[q, z], P5, (chip + r) % CHIPS * 2 + c).start()
        return carry

    lax.fori_loop(1, CHIPS, send_5, 0)
    ready(14, 20)
    arrived(racc.at[pl.ds(0, CHIPS - 1)], P5)
    for b in range(8):
        cols = jnp.concatenate([gat[2 * b].reshape(128, 128), gat[2 * b + 1].reshape(128, 128)], axis=1)
        got = dot(picks, cols)
        mine[:, b * 256 : b * 256 + 256] = got[:SLOTS]
        theirs[:, b * 256 : b * 256 + 256] = got[SLOTS:].astype(BF16)
    remote(theirs, picked, PX, mate).start()
    arrived(picked, PX)
    mixed = mine[...] + picked[...].astype(F32)
    moe = rms(mixed, mgain[...], 1e-6).astype(BF16)
    hid = (jax.nn.silu(dot(moe, gate[...])) * dot(moe, up[...])).astype(BF16)
    answer = dot(hid, down[...]).astype(BF16).astype(F32) * weight
    for b in range(8):
        ans[b * SLOTS : b * SLOTS + SLOTS, :] = answer[:, b * 256 : b * 256 + 256].astype(BF16)
    remote(ans, ans_x, AX, mate).start()
    hid = (jax.nn.silu(dot(moe, sg[...])) * dot(moe, su[...])).astype(BF16)
    shared = dot(hid[OWN:], sd[...])
    arrived(ans_x, AX)
    for k in (2, 1, 3, 0):
        zz = (z + k) % 4
        lines = pl.ds(pl.multiple_of(zz * 16, 16), 16)
        tiles = dot(spread[0, lines].reshape(256, 256), ans[...]) + dot(spread[1, lines].reshape(256, 256), ans_x[...])
        res[lines] = tiles.astype(BF16).reshape(16, 16, 256)

        def send_6(r, carry):
            t = zz * 16 + (q + r) % 16
            remote(res.at[t], racc.at[chip], P6, t * 2 + c).start()
            return carry

        lax.fori_loop(0 if k else 1, 16, send_6, 0)
    racc[chip] = res[chip]
    left(wbuf.at[pl.ds(0, 496), :], W)
    left(obuf.at[pl.ds(0, 63), 0], O)
    left(obuf.at[:, 0], OX)
    left(hbuf.at[pl.ds(0, 15)], HID)
    left(r1.at[pl.ds(0, 31)], P1)
    left(r2.at[pl.ds(0, 31)], P2)
    left(r3.at[pl.ds(0, 15)], P3)
    left(racc.at[pl.ds(0, CHIPS - 1)], P5)
    left(picked, PX)
    left(ans_x, AX)
    arrived(racc.at[pl.ds(0, CHIPS - 1)], P6)

    def add(i, carry):
        return carry + racc[i].astype(F32)

    total = lax.fori_loop(0, CHIPS, add, jnp.zeros((16, 256), F32), unroll=8)
    for s in range(2):
        for b in range(8):
            fin[s : s + 1, b * 256 : b * 256 + 256] = total[s * 8 + b : s * 8 + b + 1]
    out[:, 0:D] = (mixed[OWN : OWN + 2] + fin[...] + shared[0:2]).astype(BF16)
    left(racc.at[pl.ds(0, CHIPS - 1)], P6)


def on_device(
    hidden_in, lengths, key_cache, value_cache, query_w, key_w, value_w, out_w, lam_heads, head_gain,
    attn_gain, moe_gain, routing, route_weight, gate_w, up_w, down_w, shared_gate, shared_up, shared_down,
):
    hbm = pl.BlockSpec(memory_space=pl.ANY)
    scratch = [
        ((2, D), BF16), ((1, 8), F32), ((1, 256), F32), ((1, D), F32), ((1, D), F32),
        ((6, 256), jnp.int32), ((6, 256), F32),
        ((16, 3072), BF16), ((16, D), BF16), ((512, 384), BF16), ((CHIPS, 2, 16, 128), BF16),
        ((2, CACHE, 512), BF16), ((2, CACHE, 512), BF16),
        ((D, 512), BF16), ((D, 512), BF16), ((512, D), BF16),
        ((D, 512), BF16), ((D, 512), BF16), ((512, D), BF16),
        ((16, 2, 128), F32), ((16, 2, 128), F32), ((32, 128), F32),
        ((4, 2, 512), F32), ((32, 2, 512), F32), ((64, 512), F32), ((64, 384), F32),
        ((32, 2, 384), F32), ((32, 2, 384), F32),
        ((2, 16, 128), F32), ((2, 4, 128), F32), ((2, 2, 256), F32),
        ((2, 16, 128), F32), ((2, 16, 128), BF16), ((16, 2, 16, 128), BF16), ((512, 128), F32),
        ((32, 128), BF16), ((16, 4, 32, 128), BF16), ((2, 128, 256), F32), ((2, CHIPS, 16, 256), BF16),
        ((SLOTS, D), F32), ((SLOTS, D), BF16), ((SLOTS, D), BF16),
        ((256, 256), BF16), ((256, 256), BF16), ((CHIPS, 16, 256), BF16), ((CHIPS, 16, 256), BF16), ((2, D), F32),
    ]
    packed = pl.pallas_call(
        kernel,
        out_shape=jax.ShapeDtypeStruct((2, D + 1024), BF16),
        in_specs=[hbm] * 20,
        out_specs=pl.BlockSpec(memory_space=pltpu.VMEM),
        scratch_shapes=[pltpu.SMEM((2,), jnp.int32)]
        + [pltpu.VMEM(*s) for s in scratch]
        + [pltpu.SemaphoreType.DMA((20,)), pltpu.SemaphoreType.DMA((11,)), pltpu.SemaphoreType.DMA((11,))],
        compiler_params=pltpu.CompilerParams(
            collective_id=0, has_side_effects=True, vmem_limit_bytes=60 * 1024 * 1024
        ),
    )(
        lengths, hidden_in, lam_heads.reshape(1, 8), head_gain.reshape(1, 256),
        attn_gain.reshape(1, D), moe_gain.reshape(1, D), routing.T, route_weight.T,
        query_w, key_w, value_w, out_w, key_cache, value_cache, gate_w, up_w, down_w,
        shared_gate, shared_up, shared_down,
    )
    return packed[:, :D], packed[:, D : D + 512], packed[:, D + 512 :]


def solution(mesh):
    e2, e3 = P("ep", None), P("ep", None, None)
    return jax.shard_map(
        on_device,
        mesh=mesh,
        in_specs=(
            e2, P("ep"), e3, e3, e2, e2, e2, e2, P(), P(), P(), P(), P(), P(), e3, e3, e3, P(), P(), P(),
        ),
        out_specs=(e2, e2, e2),
        check_vma=False,
    )
```

```python
import jax
import jax.numpy as jnp
from jax import lax
from jax.experimental import pallas as pl
from jax.experimental.pallas import tpu as pltpu
from jax.sharding import PartitionSpec as P

F32 = jnp.float32
BF16 = jnp.bfloat16
MESH = pl.DeviceIdType.MESH
N = 128
CHIPS = 64
D = 2048
CACHE = 1024
SLOTS = 32
OWN = 24
W, O, OX, HID, P1, P2, P3, P5, PX, AX, P6 = range(11)


def dot(a, b):
    return jnp.dot(a, b, preferred_element_type=F32)


def dot_nt(a, b):
    return lax.dot_general(a, b, (((1,), (1,)), ((), ())), preferred_element_type=F32)


def rem(a, b):
    return lax.rem(a, jnp.int32(b))


def div(a, b):
    return lax.div(a, jnp.int32(b))


def far(pair):
    return -sum(min(k, 4 - k) for k in pair)


NEAR = sorted(((a, b) for a in range(4) for b in range(4)), key=far)
ALL = sorted(((a, b, k) for a in range(4) for b in range(4) for k in range(4)), key=far)[:-1]


def iota(shape, dim):
    return lax.broadcasted_iota(jnp.int32, shape, dim)


def rms(x, gain, eps):
    return x * lax.rsqrt(jnp.mean(x * x, axis=-1, keepdims=True) + eps) * gain


def kernel(
    lengths_h, hidden_h, lam_h, hgain_h, again_h, mgain_h, routing_h, rweight_h,
    qw, kw, vw, ow, kc_h, vc_h, gate_h, up_h, down_h, sg_h, su_h, sd_h,
    out,
    lengths, hidden, lam, hgain, again, mgain, routing, rweight,
    wcat, obuf_s, wbuf, obuf, kc, vc, gate, up, down, sg, su, sd,
    hs, hbuf, hb, s1f, s1, r1, x1, part, s2, r2, qscr, kscr, vscr, at16, s3, r3, x3,
    am, gat, pt8, spread, mine, theirs, picked, ans, ans_x, res, racc, fin,
    loc, snd, rcv, met,
):
    me = lax.axis_index("ep")
    z = div(me, 32)
    plane = rem(me, 32)
    y = div(plane, 8)
    xc = rem(me, 8)
    c = rem(me, 2)
    chip = div(me, 2)
    q = rem(chip, 16)
    slab = z * 8 + xc
    mate = me + 1 - 2 * c

    x = div(xc, 2)
    z_at = [rem(z + k, 4) for k in range(4)]
    y_at = [rem(y + k, 4) for k in range(4)]
    x_at = [rem(x + k, 4) for k in range(4)]
    plane_peers = [(dy, dx, cc) for dy, dx in NEAR for cc in (c, 1 - c)][:-2] + [(0, 0, 1 - c)]
    plane_peers = [y_at[dy] * 8 + x_at[dx] * 2 + cc for dy, dx, cc in plane_peers]
    slab_peers = [(dz, dx, cc) for dz, dx in NEAR for cc in (c, 1 - c)][:-2] + [(0, 0, 1 - c)]
    far_peers = [(z_at[dz], x_at[dx] * 2 + cc) for dz, dx, cc in slab_peers if dz]
    slab_peers = [(z_at[dz], x_at[dx] * 2 + cc) for dz, dx, cc in slab_peers]
    chips = [z_at[dz] * 16 + y_at[dy] * 4 + x_at[dx] for dz, dy, dx in ALL]

    barrier = pltpu.get_barrier_semaphore()

    def greet(semaphore, device):
        pl.semaphore_signal(semaphore, inc=1, device_id=(device,), device_id_type=MESH)

    for zt, xt in far_peers:
        greet(barrier, zt * 32 + y * 8 + xt)
    for t in plane_peers:
        greet(barrier, z * 32 + t)

    pairs = [
        (hidden_h, hidden), (again_h, again),
        (qw, wcat.at[:, pl.ds(0, 2048)]), (kw, wcat.at[:, pl.ds(2048, 512)]), (vw, wcat.at[:, pl.ds(2560, 512)]),
        (routing_h, routing), (rweight_h, rweight), (ow, obuf_s),
        (kc_h, kc), (vc_h, vc), (lengths_h, lengths), (lam_h, lam), (hgain_h, hgain), (mgain_h, mgain),
        (gate_h.at[0], gate), (up_h.at[0], up), (down_h.at[0], down), (sg_h, sg), (su_h, su), (sd_h, sd),
    ]
    copies = [pltpu.make_async_copy(src, dst, loc.at[i]) for i, (src, dst) in enumerate(pairs)]
    for copy in copies:
        copy.start()

    def ready(lo, hi):
        for copy in copies[lo:hi]:
            copy.wait()

    def remote(src, dst, phase, device):
        return pltpu.make_async_remote_copy(
            src_ref=src, dst_ref=dst, send_sem=snd.at[phase], recv_sem=rcv.at[phase],
            device_id=(device,), device_id_type=MESH,
        )

    def arrived(ref, phase):
        remote(ref, ref, phase, mate).wait_recv()

    def left(ref, phase):
        remote(ref, ref, phase, mate).wait_send()

    ready(0, 2)
    h32 = hidden[...].astype(F32)
    normed = rms(h32, again[...], 1e-6).astype(BF16).astype(F32)
    for yy in range(4):
        for zz in range(4):
            for i in range(2):
                at = zz * 512 + yy * 128
                s1f[yy, i * 4 + zz : i * 4 + zz + 1, :] = normed[i : i + 1, at : at + 128]
    s1[...] = s1f[...].astype(BF16)
    for j in range(16):
        hs[j] = h32[:, j * 128 : j * 128 + 128]
    ready(2, 5)
    pl.semaphore_wait(barrier, 55)

    at = pl.multiple_of(slab * 16, 16)
    for zt, xt in slab_peers:
        col = pl.multiple_of(xt * 384, 128)
        remote(wcat.at[:, pl.ds(col, 384)], wbuf.at[pl.ds(at, 16), :], W, zt * 32 + y * 8 + xt).start()
    for t in plane_peers:
        remote(s1.at[div(t, 8)], r1.at[plane], P1, z * 32 + t).start()
    for t in plane_peers:
        greet(met, z * 32 + t)
    own = pl.ds(pl.multiple_of(slab * 16, 16), 16)
    wbuf[own, :] = wcat[:, pl.ds(pl.multiple_of(xc * 384, 128), 384)]
    r1[plane] = s1[y]
    hbuf[q] = hs[q]

    ready(5, 8)
    obuf[chip, c] = obuf_s[:, pl.ds(pl.multiple_of(q * 128, 128), 128)]
    sel = jnp.where(
        iota((128, 256), 1) == 4 * (iota((128, 256), 0) // 2) + 2 * c + iota((128, 256), 0) % 2, 1.0, 0.0
    ).astype(BF16)
    before = jnp.where(iota((256, 256), 0) < iota((256, 256), 1), 1.0, 0.0).astype(BF16)
    picks = []
    for i, expert in enumerate((me, mate)):
        hit = routing[...] == expert
        here = jnp.sum(jnp.where(hit, 1.0, 0.0), axis=0, keepdims=True)
        rank = dot(jnp.broadcast_to(here, (16, 256)).astype(BF16), before)[0:1]
        full = jnp.where(rank == (iota((256, 256), 0) % SLOTS).astype(F32), here, 0.0)
        pt8[i] = dot_nt(sel, full.astype(BF16))
        full = full[:SLOTS]
        if i == 0:
            weight = jnp.sum(jnp.where(hit, rweight[...], 0.0), axis=0, keepdims=True)
            weight = jnp.sum(full * weight, axis=1, keepdims=True)
        mark = (iota((SLOTS, 256), 0) - OWN == iota((SLOTS, 256), 1) - 2 * expert) & (
            iota((SLOTS, 256), 1) // 2 == expert
        )
        full = full + jnp.where(mark, 1.0, 0.0)
        picks.append(dot_nt(full.astype(BF16), sel))
    picks = jnp.concatenate(picks, axis=0).astype(BF16)
    block = (iota((16, 256), 1) // SLOTS) == (iota((16, 256), 0) % 8)
    first_token = iota((16, 256), 0) < 8

    def lay(g, carry):
        for i in range(2):
            eight = pt8[i, pl.ds(pl.multiple_of(8 * g, 8), 8), :]
            for o in range(4):
                tile = jnp.where(first_token, eight[2 * o : 2 * o + 1], eight[2 * o + 1 : 2 * o + 2])
                spread[i, 4 * g + o] = jnp.where(block, tile, 0.0).astype(BF16)
        return carry

    arrived(r1.at[pl.ds(0, 31)], P1)
    x1[...] = r1[...].astype(F32).reshape(256, 128)
    wide = jnp.concatenate([x1[pl.ds(b, 64, stride=4), :].astype(BF16) for b in range(4)], axis=1)
    arrived(wbuf.at[pl.ds(0, 496), :], W)
    part[...] = dot(wide, wbuf[...])
    for i in range(32):
        s2[i] = part[2 * i : 2 * i + 2, :]

    for t in plane_peers:
        remote(s2.at[t], r2.at[plane], P2, z * 32 + t).start()
    r2[plane] = s2[plane]
    pl.semaphore_wait(met, 31)
    for t in chips:
        col = pl.multiple_of(rem(t, 16) * 128, 128)
        remote(obuf_s.at[:, pl.ds(col, 128)], obuf.at[chip, c], O, t * 2 + c).start()
    for dy, dx in NEAR[:-1]:
        t = y_at[dy] * 4 + x_at[dx]
        remote(hs.at[t], hbuf.at[q], HID, z * 32 + t * 2 + c).start()
    lax.fori_loop(0, CHIPS // 4, lay, 0)
    arrived(r2.at[pl.ds(0, 31)], P2)

    for u in range(24):
        cb, at = u // 3, (u % 3) * 128
        val = r2[cb, :, at : at + 128]
        for yy in range(1, 4):
            val = val + r2[yy * 8 + cb, :, at : at + 128]
        for s in range(2):
            line = val[s : s + 1, :]
            if u < 16:
                r = (u % 2) * 8 + u // 2
                qscr[s, r : r + 1, :] = line
            elif u < 20:
                kscr[s, u - 16 : u - 15, :] = line
            else:
                v = u - 20
                vscr[s, v // 2 : v // 2 + 1, (v % 2) * 128 : (v % 2) * 128 + 128] = line

    ready(8, 14)
    rows = iota((16, 1), 0)
    pair_of = (rows // 8) + 2 * ((rows % 8) // 4)
    first = iota((8, 1), 0) < 4
    lam_col = jnp.sum(jnp.where(iota((8, 8), 0) == iota((8, 8), 1), lam[...], 0.0), axis=1, keepdims=True)
    scale = 128 ** (-0.5)
    place = iota((1, CACHE), 1)
    lane = iota((1, 128), 1)
    inverse = jnp.exp((lane % 64).astype(F32) * (-13.122363377404328 / 64))
    for s in range(2):
        angle = lengths[s].astype(F32) * inverse
        cos_row = jnp.cos(angle)
        sin_row = jnp.where(lane < 64, -jnp.sin(angle), jnp.sin(angle))

        def turn(v):
            return (v * cos_row + pltpu.roll(v, 64, 1) * sin_row).astype(BF16)

        qq = turn(qscr[s]).astype(F32)
        kn = turn(kscr[s])
        vn = vscr[s].astype(BF16)
        for u in range(4):
            out[s : s + 1, D + u * 128 : D + u * 128 + 128] = kn[u : u + 1]
        for u in range(2):
            out[s : s + 1, D + 512 + u * 256 : D + 512 + u * 256 + 256] = vn[u : u + 1]
        kn = kn.astype(F32)
        vn = vn.astype(F32)
        wide = jnp.concatenate([jnp.where(pair_of == u, qq, 0.0) for u in range(4)], axis=1).astype(BF16)
        scores = dot_nt(wide, kc[s]) * scale
        k_of = jnp.where(
            pair_of == 0, kn[0:1], jnp.where(pair_of == 1, kn[1:2], jnp.where(pair_of == 2, kn[2:3], kn[3:4]))
        )
        own_score = jnp.sum(qq * k_of, axis=1, keepdims=True) * scale
        live = place < lengths[s]
        peak = jnp.maximum(jnp.max(jnp.where(live, scores, -jnp.inf), axis=1, keepdims=True), own_score)
        weights = jnp.where(live, jnp.exp(scores - peak), 0.0)
        own_weight = jnp.exp(own_score - peak)
        totals = jnp.sum(weights, axis=1, keepdims=True) + own_weight
        share = 1.0 / totals
        maps = weights * share
        own_maps = own_weight * share
        combined = (maps[:8] - lam_col * maps[8:]).astype(BF16)
        own_comb = (own_maps[:8] - lam_col * own_maps[8:]).astype(BF16).astype(F32)
        both = dot(combined, vc[s])
        head_out = jnp.where(first, both[:, :256], both[:, 256:])
        head_out = head_out + own_comb * jnp.where(first, vn[0:1], vn[1:2])
        att = rms(head_out, hgain[...], 1e-5)
        for h in range(8):
            for half in range(2):
                at16[s, 2 * h + half : 2 * h + half + 1, :] = att[h : h + 1, half * 128 : half * 128 + 128]
        s3[s] = at16[s].astype(BF16)

    for dy, dx in NEAR[:-1]:
        t = y_at[dy] * 4 + x_at[dx]
        remote(s3, r3.at[q], P3, z * 32 + t * 2 + c).start()
    r3[q] = s3[...]
    arrived(obuf.at[pl.ds(0, 63), 0], O)
    remote(obuf.at[:, c], obuf.at[:, c], OX, mate).start()
    arrived(hbuf.at[pl.ds(0, 15)], HID)
    for i in range(16):
        hb[2 * i : 2 * i + 2, :] = hbuf[i]
    arrived(obuf.at[:, 0], OX)
    arrived(r3.at[pl.ds(0, 15)], P3)
    x3[...] = r3[...].reshape(512, 128).astype(F32)
    wide = jnp.concatenate([x3[pl.ds(b, 32, stride=16), :].astype(BF16) for b in range(16)], axis=1)
    proj = dot(wide, obuf[...].reshape(D, 128))
    mixed = (hb[...] + proj.astype(BF16).astype(F32)).astype(BF16)
    am[...] = mixed
    gat[q, z] = mixed

    for t in chips:
        remote(am, gat.at[q, z], P5, t * 2 + c).start()
    ready(14, 20)
    arrived(racc.at[pl.ds(0, CHIPS - 1)], P5)
    for b in range(8):
        cols = jnp.concatenate([gat[2 * b].reshape(128, 128), gat[2 * b + 1].reshape(128, 128)], axis=1)
        got = dot(picks, cols)
        mine[:, b * 256 : b * 256 + 256] = got[:SLOTS]
        theirs[:, b * 256 : b * 256 + 256] = got[SLOTS:].astype(BF16)
    remote(theirs, picked, PX, mate).start()
    arrived(picked, PX)
    mixed = mine[...] + picked[...].astype(F32)
    moe = rms(mixed, mgain[...], 1e-6).astype(BF16)
    hid = (jax.nn.silu(dot(moe, gate[...])) * dot(moe, up[...])).astype(BF16)
    answer = dot(hid, down[...]).astype(BF16).astype(F32) * weight
    for b in range(8):
        ans[b * SLOTS : b * SLOTS + SLOTS, :] = answer[:, b * 256 : b * 256 + 256].astype(BF16)
    remote(ans, ans_x, AX, mate).start()
    arrived(ans_x, AX)
    for k in (2, 1, 3, 0):
        lines = pl.ds(pl.multiple_of(z_at[k] * 16, 16), 16)
        tiles = dot(spread[0, lines].reshape(256, 256), ans[...]) + dot(spread[1, lines].reshape(256, 256), ans_x[...])
        res[lines] = tiles.astype(BF16).reshape(16, 16, 256)
        for dy, dx in NEAR if k else NEAR[:-1]:
            t = z_at[k] * 16 + y_at[dy] * 4 + x_at[dx]
            remote(res.at[t], racc.at[chip], P6, t * 2 + c).start()
    racc[chip] = res[chip]
    hid = (jax.nn.silu(dot(moe, sg[...])) * dot(moe, su[...])).astype(BF16)
    shared = dot(hid[OWN:], sd[...])
    left(wbuf.at[pl.ds(0, 496), :], W)
    left(obuf.at[pl.ds(0, 63), 0], O)
    left(obuf.at[:, 0], OX)
    left(hbuf.at[pl.ds(0, 15)], HID)
    left(r1.at[pl.ds(0, 31)], P1)
    left(r2.at[pl.ds(0, 31)], P2)
    left(r3.at[pl.ds(0, 15)], P3)
    left(racc.at[pl.ds(0, CHIPS - 1)], P5)
    left(picked, PX)
    left(ans_x, AX)
    arrived(racc.at[pl.ds(0, CHIPS - 1)], P6)

    def add(i, carry):
        return carry + racc[i].astype(F32)

    total = lax.fori_loop(0, CHIPS, add, jnp.zeros((16, 256), F32), unroll=8)
    for s in range(2):
        for b in range(8):
            fin[s : s + 1, b * 256 : b * 256 + 256] = total[s * 8 + b : s * 8 + b + 1]
    out[:, 0:D] = (mixed[OWN : OWN + 2] + fin[...] + shared[0:2]).astype(BF16)
    left(racc.at[pl.ds(0, CHIPS - 1)], P6)


def on_device(
    hidden_in, lengths, key_cache, value_cache, query_w, key_w, value_w, out_w, lam_heads, head_gain,
    attn_gain, moe_gain, routing, route_weight, gate_w, up_w, down_w, shared_gate, shared_up, shared_down,
):
    hbm = pl.BlockSpec(memory_space=pl.ANY)
    scratch = [
        ((2, D), BF16), ((1, 8), F32), ((1, 256), F32), ((1, D), F32), ((1, D), F32),
        ((6, 256), jnp.int32), ((6, 256), F32),
        ((16, 3072), BF16), ((16, D), BF16), ((512, 384), BF16), ((CHIPS, 2, 16, 128), BF16),
        ((2, CACHE, 512), BF16), ((2, CACHE, 512), BF16),
        ((D, 512), BF16), ((D, 512), BF16), ((512, D), BF16),
        ((D, 512), BF16), ((D, 512), BF16), ((512, D), BF16),
        ((16, 2, 128), F32), ((16, 2, 128), F32), ((32, 128), F32),
        ((4, 8, 128), F32), ((4, 8, 128), BF16), ((32, 8, 128), BF16), ((256, 128), F32), ((64, 384), F32),
        ((32, 2, 384), F32), ((32, 2, 384), F32),
        ((2, 16, 128), F32), ((2, 4, 128), F32), ((2, 2, 256), F32),
        ((2, 16, 128), F32), ((2, 16, 128), BF16), ((16, 2, 16, 128), BF16), ((512, 128), F32),
        ((32, 128), BF16), ((16, 4, 32, 128), BF16), ((2, 128, 256), F32), ((2, CHIPS, 16, 256), BF16),
        ((SLOTS, D), F32), ((SLOTS, D), BF16), ((SLOTS, D), BF16),
        ((256, 256), BF16), ((256, 256), BF16), ((CHIPS, 16, 256), BF16), ((CHIPS, 16, 256), BF16), ((2, D), F32),
    ]
    packed = pl.pallas_call(
        kernel,
        out_shape=jax.ShapeDtypeStruct((2, D + 1024), BF16),
        in_specs=[hbm] * 20,
        out_specs=pl.BlockSpec(memory_space=pltpu.VMEM),
        scratch_shapes=[pltpu.SMEM((2,), jnp.int32)]
        + [pltpu.VMEM(*s) for s in scratch]
        + [pltpu.SemaphoreType.DMA((20,)), pltpu.SemaphoreType.DMA((11,)), pltpu.SemaphoreType.DMA((11,))]
        + [pltpu.SemaphoreType.REGULAR],
        compiler_params=pltpu.CompilerParams(
            collective_id=0, has_side_effects=True, vmem_limit_bytes=60 * 1024 * 1024
        ),
    )(
        lengths, hidden_in, lam_heads.reshape(1, 8), head_gain.reshape(1, 256),
        attn_gain.reshape(1, D), moe_gain.reshape(1, D), routing.T, route_weight.T,
        query_w, key_w, value_w, out_w, key_cache, value_cache, gate_w, up_w, down_w,
        shared_gate, shared_up, shared_down,
    )
    return packed[:, :D], packed[:, D : D + 512], packed[:, D + 512 :]


def solution(mesh):
    e2, e3 = P("ep", None), P("ep", None, None)
    return jax.shard_map(
        on_device,
        mesh=mesh,
        in_specs=(
            e2, P("ep"), e3, e3, e2, e2, e2, e2, P(), P(), P(), P(), P(), P(), e3, e3, e3, P(), P(), P(),
        ),
        out_specs=(e2, e2, e2),
        check_vma=False,
    )
```

```python
import jax
import jax.numpy as jnp
from jax import lax
from jax.experimental import pallas as pl
from jax.experimental.pallas import tpu as pltpu
from jax.sharding import PartitionSpec as P

F32 = jnp.float32
BF16 = jnp.bfloat16
MESH = pl.DeviceIdType.MESH
N = 128
CHIPS = 64
D = 2048
CACHE = 1024
SLOTS = 32
OWN = 24
W, O, OX, HID, P1, P2, P3, P5, PX, AX, P6 = range(11)


def dot(a, b):
    return jnp.dot(a, b, preferred_element_type=F32)


def dot_nt(a, b):
    return lax.dot_general(a, b, (((1,), (1,)), ((), ())), preferred_element_type=F32)


def rem(a, b):
    return lax.rem(a, jnp.int32(b))


def div(a, b):
    return lax.div(a, jnp.int32(b))


def far(pair):
    return -sum(min(k, 4 - k) for k in pair)


NEAR = sorted(((a, b) for a in range(4) for b in range(4)), key=far)
ALL = sorted(((a, b, k) for a in range(4) for b in range(4) for k in range(4)), key=far)[:-1]


def iota(shape, dim):
    return lax.broadcasted_iota(jnp.int32, shape, dim)


def rms(x, gain, eps):
    return x * lax.rsqrt(jnp.mean(x * x, axis=-1, keepdims=True) + eps) * gain


def kernel(
    lengths_h, hidden_h, lam_h, hgain_h, again_h, mgain_h, routing_h, rweight_h,
    qw, kw, vw, ow, kc_h, vc_h, gate_h, up_h, down_h, sg_h, su_h, sd_h,
    out,
    lengths, hidden, lam, hgain, again, mgain, routing, rweight,
    wcat, obuf_s, wbuf, obuf, kc, vc, gate, up, down, sg, su, sd,
    hs, hbuf, hb, s1f, s1, r1, x1, part, s2, r2, qscr, kscr, vscr, at16, s3, r3, x3,
    am, gat, spread, mine, theirs, picked, ans, res, racc, fin,
    loc, snd, rcv, met,
):
    me = lax.axis_index("ep")
    z = div(me, 32)
    plane = rem(me, 32)
    y = div(plane, 8)
    xc = rem(me, 8)
    c = rem(me, 2)
    chip = div(me, 2)
    q = rem(chip, 16)
    slab = z * 8 + xc
    mate = me + 1 - 2 * c

    x = div(xc, 2)
    z_at = [rem(z + k, 4) for k in range(4)]
    y_at = [rem(y + k, 4) for k in range(4)]
    x_at = [rem(x + k, 4) for k in range(4)]
    plane_peers = [(dy, dx, cc) for dy, dx in NEAR for cc in (c, 1 - c)][:-2] + [(0, 0, 1 - c)]
    plane_peers = [y_at[dy] * 8 + x_at[dx] * 2 + cc for dy, dx, cc in plane_peers]
    slab_peers = [(dz, dx, cc) for dz, dx in NEAR for cc in (c, 1 - c)][:-2] + [(0, 0, 1 - c)]
    far_peers = [(z_at[dz], x_at[dx] * 2 + cc) for dz, dx, cc in slab_peers if dz]
    slab_peers = [(z_at[dz], x_at[dx] * 2 + cc) for dz, dx, cc in slab_peers]
    chips = [z_at[dz] * 16 + y_at[dy] * 4 + x_at[dx] for dz, dy, dx in ALL]

    barrier = pltpu.get_barrier_semaphore()

    def greet(semaphore, device):
        pl.semaphore_signal(semaphore, inc=1, device_id=(device,), device_id_type=MESH)

    for zt, xt in far_peers:
        greet(barrier, zt * 32 + y * 8 + xt)
    for t in plane_peers:
        greet(barrier, z * 32 + t)

    pairs = [
        (hidden_h, hidden), (again_h, again),
        (qw, wcat.at[:, pl.ds(0, 2048)]), (kw, wcat.at[:, pl.ds(2048, 512)]), (vw, wcat.at[:, pl.ds(2560, 512)]),
        (routing_h, routing), (rweight_h, rweight), (ow, obuf_s),
        (kc_h, kc), (vc_h, vc), (lengths_h, lengths), (lam_h, lam), (hgain_h, hgain), (mgain_h, mgain),
        (gate_h.at[0], gate), (up_h.at[0], up), (down_h.at[0], down), (sg_h, sg), (su_h, su), (sd_h, sd),
    ]
    copies = [pltpu.make_async_copy(src, dst, loc.at[i]) for i, (src, dst) in enumerate(pairs)]
    for copy in copies:
        copy.start()

    def ready(lo, hi):
        for copy in copies[lo:hi]:
            copy.wait()

    def remote(src, dst, phase, device):
        return pltpu.make_async_remote_copy(
            src_ref=src, dst_ref=dst, send_sem=snd.at[phase], recv_sem=rcv.at[phase],
            device_id=(device,), device_id_type=MESH,
        )

    def arrived(ref, phase):
        remote(ref, ref, phase, mate).wait_recv()

    def left(ref, phase):
        remote(ref, ref, phase, mate).wait_send()

    ready(0, 2)
    h32 = hidden[...].astype(F32)
    normed = rms(h32, again[...], 1e-6).astype(BF16).astype(F32)
    for yy in range(4):
        for zz in range(4):
            for i in range(2):
                at = zz * 512 + yy * 128
                s1f[yy, i * 4 + zz : i * 4 + zz + 1, :] = normed[i : i + 1, at : at + 128]
    s1[...] = s1f[...].astype(BF16)
    for j in range(16):
        hs[j] = h32[:, j * 128 : j * 128 + 128]
    ready(2, 5)
    pl.semaphore_wait(barrier, 55)

    at = pl.multiple_of(slab * 16, 16)
    for zt, xt in slab_peers:
        col = pl.multiple_of(xt * 384, 128)
        remote(wcat.at[:, pl.ds(col, 384)], wbuf.at[pl.ds(at, 16), :], W, zt * 32 + y * 8 + xt).start()
    for t in plane_peers:
        remote(s1.at[div(t, 8)], r1.at[plane], P1, z * 32 + t).start()
    for t in plane_peers:
        greet(met, z * 32 + t)
    own = pl.ds(pl.multiple_of(slab * 16, 16), 16)
    wbuf[own, :] = wcat[:, pl.ds(pl.multiple_of(xc * 384, 128), 384)]
    r1[plane] = s1[y]
    hbuf[q] = hs[q]

    ready(5, 8)
    obuf[chip, c] = obuf_s[:, pl.ds(pl.multiple_of(q * 128, 128), 128)]
    sel = jnp.where(
        iota((128, 256), 1) == 4 * (iota((128, 256), 0) // 2) + 2 * c + iota((128, 256), 0) % 2, 1.0, 0.0
    ).astype(BF16)
    before = jnp.where(iota((256, 256), 0) < iota((256, 256), 1), 1.0, 0.0).astype(BF16)
    picks, back = [], []
    for i, expert in enumerate((me, mate)):
        hit = routing[...] == expert
        here = jnp.sum(jnp.where(hit, 1.0, 0.0), axis=0, keepdims=True)
        rank = dot(jnp.broadcast_to(here, (16, 256)).astype(BF16), before)[0:1]
        full = jnp.where(rank == iota((SLOTS, 256), 0).astype(F32), here, 0.0)
        back.append(dot_nt(sel, full.astype(BF16)))
        if i == 0:
            weight = jnp.sum(jnp.where(hit, rweight[...], 0.0), axis=0, keepdims=True)
            weight = jnp.sum(full * weight, axis=1, keepdims=True)
        mark = (iota((SLOTS, 256), 0) - OWN == iota((SLOTS, 256), 1) - 2 * expert) & (
            iota((SLOTS, 256), 1) // 2 == expert
        )
        full = full + jnp.where(mark, 1.0, 0.0)
        picks.append(dot_nt(full.astype(BF16), sel))
    picks = jnp.concatenate(picks, axis=0).astype(BF16)
    back = jnp.concatenate(back, axis=1).astype(BF16)

    arrived(r1.at[pl.ds(0, 31)], P1)
    x1[...] = r1[...].astype(F32).reshape(256, 128)
    wide = jnp.concatenate([x1[pl.ds(b, 64, stride=4), :].astype(BF16) for b in range(4)], axis=1)
    arrived(wbuf.at[pl.ds(0, 496), :], W)
    part[...] = dot(wide, wbuf[...])
    for i in range(32):
        s2[i] = part[2 * i : 2 * i + 2, :]

    for t in plane_peers:
        remote(s2.at[t], r2.at[plane], P2, z * 32 + t).start()
    r2[plane] = s2[plane]
    pl.semaphore_wait(met, 31)
    for t in chips:
        col = pl.multiple_of(rem(t, 16) * 128, 128)
        remote(obuf_s.at[:, pl.ds(col, 128)], obuf.at[chip, c], O, t * 2 + c).start()
    for dy, dx in NEAR[:-1]:
        t = y_at[dy] * 4 + x_at[dx]
        remote(hs.at[t], hbuf.at[q], HID, z * 32 + t * 2 + c).start()
    arrived(r2.at[pl.ds(0, 31)], P2)

    for u in range(24):
        cb, at = u // 3, (u % 3) * 128
        val = r2[cb, :, at : at + 128]
        for yy in range(1, 4):
            val = val + r2[yy * 8 + cb, :, at : at + 128]
        for s in range(2):
            line = val[s : s + 1, :]
            if u < 16:
                r = (u % 2) * 8 + u // 2
                qscr[s, r : r + 1, :] = line
            elif u < 20:
                kscr[s, u - 16 : u - 15, :] = line
            else:
                v = u - 20
                vscr[s, v // 2 : v // 2 + 1, (v % 2) * 128 : (v % 2) * 128 + 128] = line

    ready(8, 14)
    rows = iota((16, 1), 0)
    pair_of = (rows // 8) + 2 * ((rows % 8) // 4)
    first = iota((8, 1), 0) < 4
    lam_col = jnp.sum(jnp.where(iota((8, 8), 0) == iota((8, 8), 1), lam[...], 0.0), axis=1, keepdims=True)
    scale = 128 ** (-0.5)
    place = iota((1, CACHE), 1)
    lane = iota((1, 128), 1)
    inverse = jnp.exp((lane % 64).astype(F32) * (-13.122363377404328 / 64))

    def turn(v, cos_row, sin_row):
        return (v * cos_row + pltpu.roll(v, 64, 1) * sin_row).astype(BF16)

    q_rows, k_rows, v_rows, all_scores = [], [], [], []
    for s in range(2):
        angle = lengths[s].astype(F32) * inverse
        cos_row = jnp.cos(angle)
        sin_row = jnp.sin(angle)
        sin_row = jnp.where(lane < 64, -sin_row, sin_row)
        qq = turn(qscr[s], cos_row, sin_row).astype(F32)
        wide = jnp.concatenate([jnp.where(pair_of == u, qq, 0.0) for u in range(4)], axis=1).astype(BF16)
        all_scores.append(dot_nt(wide, kc[s]))
        kn = turn(kscr[s], cos_row, sin_row)
        vn = vscr[s].astype(BF16)
        for u in range(4):
            out[s : s + 1, D + u * 128 : D + u * 128 + 128] = kn[u : u + 1]
        for u in range(2):
            out[s : s + 1, D + 512 + u * 256 : D + 512 + u * 256 + 256] = vn[u : u + 1]
        q_rows.append(qq)
        k_rows.append(kn.astype(F32))
        v_rows.append(vn.astype(F32))
    sums, own_parts = [], []
    for s in range(2):
        qq, kn = q_rows[s], k_rows[s]
        scores = all_scores[s] * scale
        k_of = jnp.where(
            pair_of == 0, kn[0:1], jnp.where(pair_of == 1, kn[1:2], jnp.where(pair_of == 2, kn[2:3], kn[3:4]))
        )
        own_score = jnp.sum(qq * k_of, axis=1, keepdims=True) * scale
        live = place < lengths[s]
        peak = jnp.maximum(jnp.max(jnp.where(live, scores, -jnp.inf), axis=1, keepdims=True), own_score)
        weights = jnp.where(live, jnp.exp(scores - peak), 0.0)
        own_weight = jnp.exp(own_score - peak)
        share = 1.0 / (jnp.sum(weights, axis=1, keepdims=True) + own_weight)
        maps = weights * share
        own_maps = own_weight * share
        combined = (maps[:8] - lam_col * maps[8:]).astype(BF16)
        own_parts.append((own_maps[:8] - lam_col * own_maps[8:]).astype(BF16).astype(F32))
        sums.append(dot(combined, vc[s]))
    for s in range(2):
        head_out = jnp.where(first, sums[s][:, :256], sums[s][:, 256:])
        head_out = head_out + own_parts[s] * jnp.where(first, v_rows[s][0:1], v_rows[s][1:2])
        att = rms(head_out, hgain[...], 1e-5)
        for h in range(8):
            for half in range(2):
                at16[s, 2 * h + half : 2 * h + half + 1, :] = att[h : h + 1, half * 128 : half * 128 + 128]
        s3[s] = at16[s].astype(BF16)

    for dy, dx in NEAR[:-1]:
        t = y_at[dy] * 4 + x_at[dx]
        remote(s3, r3.at[q], P3, z * 32 + t * 2 + c).start()
    r3[q] = s3[...]
    arrived(obuf.at[pl.ds(0, 63), 0], O)
    remote(obuf.at[:, c], obuf.at[:, c], OX, mate).start()
    arrived(hbuf.at[pl.ds(0, 15)], HID)
    for i in range(16):
        hb[2 * i : 2 * i + 2, :] = hbuf[i]
    arrived(obuf.at[:, 0], OX)
    arrived(r3.at[pl.ds(0, 15)], P3)
    x3[...] = r3[...].reshape(512, 128).astype(F32)
    wide = jnp.concatenate([x3[pl.ds(b, 32, stride=16), :].astype(BF16) for b in range(16)], axis=1)
    proj = dot(wide, obuf[...].reshape(D, 128))
    mixed = (hb[...] + proj.astype(BF16).astype(F32)).astype(BF16)
    am[...] = mixed
    gat[q, z] = mixed

    for t in chips:
        remote(am, gat.at[q, z], P5, t * 2 + c).start()
    ready(14, 20)
    arrived(racc.at[pl.ds(0, CHIPS - 1)], P5)
    for b in range(8):
        cols = jnp.concatenate([gat[2 * b].reshape(128, 128), gat[2 * b + 1].reshape(128, 128)], axis=1)
        got = dot(picks, cols)
        mine[:, b * 256 : b * 256 + 256] = got[:SLOTS]
        theirs[:, b * 256 : b * 256 + 256] = got[SLOTS:].astype(BF16)
    remote(theirs, picked, PX, mate).start()
    arrived(picked, PX)
    mixed = mine[...] + picked[...].astype(F32)
    moe = rms(mixed, mgain[...], 1e-6).astype(BF16)
    hid = (jax.nn.silu(dot(moe, gate[...])) * dot(moe, up[...])).astype(BF16)
    answer = dot(hid, down[...]).astype(BF16).astype(F32) * weight
    for b in range(8):
        ans[b, 0:SLOTS] = answer[:, b * 256 : b * 256 + 256].astype(BF16)
    remote(ans.at[:, pl.ds(0, SLOTS)], ans.at[:, pl.ds(SLOTS, SLOTS)], AX, mate).start()
    arrived(ans.at[:, pl.ds(0, SLOTS)], AX)
    for b in range(8):
        tiles = dot(back, ans[b])
        for half in range(2):
            spread[half, pl.ds(b, 128, stride=8), :] = tiles[:, half * 128 : half * 128 + 128]
    for k in (2, 1, 3, 0):
        lines = pl.ds(pl.multiple_of(z_at[k] * 16, 16), 16)
        rows = pl.ds(pl.multiple_of(z_at[k] * 256, 256), 256)
        tiles = jnp.concatenate([spread[0, rows, :], spread[1, rows, :]], axis=1)
        res[lines] = tiles.astype(BF16).reshape(16, 16, 256)
        for dy, dx in NEAR if k else NEAR[:-1]:
            t = z_at[k] * 16 + y_at[dy] * 4 + x_at[dx]
            remote(res.at[t], racc.at[chip], P6, t * 2 + c).start()
    racc[chip] = res[chip]
    hid = (jax.nn.silu(dot(moe, sg[...])) * dot(moe, su[...])).astype(BF16)
    shared = dot(hid[OWN:], sd[...])
    left(wbuf.at[pl.ds(0, 496), :], W)
    left(obuf.at[pl.ds(0, 63), 0], O)
    left(obuf.at[:, 0], OX)
    left(hbuf.at[pl.ds(0, 15)], HID)
    left(r1.at[pl.ds(0, 31)], P1)
    left(r2.at[pl.ds(0, 31)], P2)
    left(r3.at[pl.ds(0, 15)], P3)
    left(racc.at[pl.ds(0, CHIPS - 1)], P5)
    left(picked, PX)
    left(ans.at[:, pl.ds(0, SLOTS)], AX)
    arrived(racc.at[pl.ds(0, CHIPS - 1)], P6)

    def add(i, carry):
        return carry + racc[i].astype(F32)

    total = lax.fori_loop(0, CHIPS, add, jnp.zeros((16, 256), F32), unroll=8)
    for s in range(2):
        for b in range(8):
            fin[s : s + 1, b * 256 : b * 256 + 256] = total[s * 8 + b : s * 8 + b + 1]
    out[:, 0:D] = (mixed[OWN : OWN + 2] + fin[...] + shared[0:2]).astype(BF16)
    left(racc.at[pl.ds(0, CHIPS - 1)], P6)


def on_device(
    hidden_in, lengths, key_cache, value_cache, query_w, key_w, value_w, out_w, lam_heads, head_gain,
    attn_gain, moe_gain, routing, route_weight, gate_w, up_w, down_w, shared_gate, shared_up, shared_down,
):
    hbm = pl.BlockSpec(memory_space=pl.ANY)
    scratch = [
        ((2, D), BF16), ((1, 8), F32), ((1, 256), F32), ((1, D), F32), ((1, D), F32),
        ((6, 256), jnp.int32), ((6, 256), F32),
        ((16, 3072), BF16), ((16, D), BF16), ((512, 384), BF16), ((CHIPS, 2, 16, 128), BF16),
        ((2, CACHE, 512), BF16), ((2, CACHE, 512), BF16),
        ((D, 512), BF16), ((D, 512), BF16), ((512, D), BF16),
        ((D, 512), BF16), ((D, 512), BF16), ((512, D), BF16),
        ((16, 2, 128), F32), ((16, 2, 128), F32), ((32, 128), F32),
        ((4, 8, 128), F32), ((4, 8, 128), BF16), ((32, 8, 128), BF16), ((256, 128), F32), ((64, 384), F32),
        ((32, 2, 384), F32), ((32, 2, 384), F32),
        ((2, 16, 128), F32), ((2, 4, 128), F32), ((2, 2, 256), F32),
        ((2, 16, 128), F32), ((2, 16, 128), BF16), ((16, 2, 16, 128), BF16), ((512, 128), F32),
        ((32, 128), BF16), ((16, 4, 32, 128), BF16), ((2, 1024, 128), F32),
        ((SLOTS, D), F32), ((SLOTS, D), BF16), ((SLOTS, D), BF16),
        ((8, 2 * SLOTS, 256), BF16), ((CHIPS, 16, 256), BF16), ((CHIPS, 16, 256), BF16), ((2, D), F32),
    ]
    packed = pl.pallas_call(
        kernel,
        out_shape=jax.ShapeDtypeStruct((2, D + 1024), BF16),
        in_specs=[hbm] * 20,
        out_specs=pl.BlockSpec(memory_space=pltpu.VMEM),
        scratch_shapes=[pltpu.SMEM((2,), jnp.int32)]
        + [pltpu.VMEM(*s) for s in scratch]
        + [pltpu.SemaphoreType.DMA((20,)), pltpu.SemaphoreType.DMA((11,)), pltpu.SemaphoreType.DMA((11,))]
        + [pltpu.SemaphoreType.REGULAR],
        compiler_params=pltpu.CompilerParams(
            collective_id=0, has_side_effects=True, vmem_limit_bytes=60 * 1024 * 1024
        ),
    )(
        lengths, hidden_in, lam_heads.reshape(1, 8), head_gain.reshape(1, 256),
        attn_gain.reshape(1, D), moe_gain.reshape(1, D), routing.T, route_weight.T,
        query_w, key_w, value_w, out_w, key_cache, value_cache, gate_w, up_w, down_w,
        shared_gate, shared_up, shared_down,
    )

    def unpack(src, layer, key, value):
        layer[...] = src[:, 0:D]
        key[...] = src[:, D : D + 512]
        value[...] = src[:, D + 512 :]

    vmem = pl.BlockSpec(memory_space=pltpu.VMEM)
    return pl.pallas_call(
        unpack,
        out_shape=(
            jax.ShapeDtypeStruct((2, D), BF16),
            jax.ShapeDtypeStruct((2, 512), BF16),
            jax.ShapeDtypeStruct((2, 512), BF16),
        ),
        in_specs=[vmem],
        out_specs=(vmem, vmem, vmem),
        compiler_params=pltpu.CompilerParams(vmem_limit_bytes=60 * 1024 * 1024),
    )(packed)


def solution(mesh):
    e2, e3 = P("ep", None), P("ep", None, None)
    return jax.shard_map(
        on_device,
        mesh=mesh,
        in_specs=(
            e2, P("ep"), e3, e3, e2, e2, e2, e2, P(), P(), P(), P(), P(), P(), e3, e3, e3, P(), P(), P(),
        ),
        out_specs=(e2, e2, e2),
        check_vma=False,
    )
```

```python
import jax
import jax.numpy as jnp
from jax import lax
from jax.experimental import pallas as pl
from jax.experimental.pallas import tpu as pltpu
from jax.sharding import PartitionSpec as P

F32 = jnp.float32
BF16 = jnp.bfloat16
MESH = pl.DeviceIdType.MESH
N = 128
CHIPS = 64
D = 2048
CACHE = 1024
SLOTS = 32
OWN = 24
W, O, OX, HID, P1, P2, P3, P5, GX, UX, DX, P6 = range(12)


def dot(a, b):
    return jnp.dot(a, b, preferred_element_type=F32)


def dot_nt(a, b):
    return lax.dot_general(a, b, (((1,), (1,)), ((), ())), preferred_element_type=F32)


def rem(a, b):
    return lax.rem(a, jnp.int32(b))


def div(a, b):
    return lax.div(a, jnp.int32(b))


def kind(v):
    return rem(div(v + 1, 2), 2)


def far(pair):
    return -sum(min(k, 4 - k) for k in pair)


NEAR = sorted(((a, b) for a in range(4) for b in range(4)), key=far)
ALL = sorted(((a, b, k) for a in range(4) for b in range(4) for k in range(4)), key=far)[:-1]


def iota(shape, dim):
    return lax.broadcasted_iota(jnp.int32, shape, dim)


def rms(x, gain, eps):
    return x * lax.rsqrt(jnp.mean(x * x, axis=-1, keepdims=True) + eps) * gain


def kernel(
    lengths_h, hidden_h, lam_h, hgain_h, again_h, mgain_h, routing_h, rweight_h,
    qw, kw, vw, ow, kc_h, vc_h, gate_h, up_h, down_h, sg_h, su_h, sd_h,
    out,
    lengths, hidden, lam, hgain, again, mgain, routing, rweight,
    wcat, obuf_s, wbuf, obuf, kc, vc, gate, up, down, gate_x, up_x, down_x, sg, su, sd,
    hs, hbuf, hb, lines, s1f, s1, r1, x1, part, s2, r2, qscr, kscr, vscr, at16, s3, r3, x3,
    am, gat, spread, mine, ans, res, racc, fin,
    loc, snd, rcv, met,
):
    me = lax.axis_index("ep")
    z = div(me, 32)
    y = rem(div(me, 8), 4)
    xc = rem(me, 8)
    c = rem(me, 2)
    chip = div(me, 2)
    q = rem(chip, 16)
    mate = me + 1 - 2 * c

    x = div(xc, 2)
    z_at = [rem(z + k, 4) for k in range(4)]
    y_at = [rem(y + k, 4) for k in range(4)]
    x_at = [rem(x + k, 4) for k in range(4)]
    flips = sorted(((a, b, k, e) for a in (0, 1) for b in (0, 1) for k in (0, 1) for e in (0, 1)), key=sum)[:0:-1]
    hops = sorted(
        ((a, b, k, e) for a in range(4) for b in (0, 1) for k in (0, 1) for e in (0, 1)),
        key=lambda h: -(min(h[0], 4 - h[0]) + h[1] + h[2] + 0.1 * h[3]),
    )[:-1]
    cube_peers, cube_row, cube_col, group_peers, seat, my_kind = [], [], [], [], [], []
    for h in range(2):
        zs, ys, xs = (rem(v + h, 4) for v in (z, y, x))
        zo, yo, xo = (rem(7 - v - h, 4) for v in (zs, ys, xs))
        long, pair = (zs, xs) if h == 0 else (xs, zs)
        peers = []
        for a, b, k, e in flips:
            zt, yt, xt, ct = (z, zo)[a], (y, yo)[b], (x, xo)[k], (c, 1 - c)[e]
            lt = rem((zt, xt)[h] + h, 4)
            col = pl.multiple_of(h * 1536 + (div(lt, 2) * 2 + ct) * 384, 128)
            peers.append((zt * 32 + yt * 8 + xt * 2 + ct, col))
        cube_peers.append(peers)
        at = div(zs, 2) * 128 + div(ys, 2) * 64 + c * 16
        cube_row.append(pl.multiple_of(at + 32 * jnp.where(kind(xs) == 1, div(xs, 2), 1 - div(xs, 2)), 16))
        cube_col.append(pl.multiple_of(h * 1536 + (div(long, 2) * 2 + c) * 384, 128))
        seat.append(((long * 2 + rem(ys, 2)) * 2 + rem(pair, 2)) * 2 + c)
        my_kind.append((kind(zs) * 2 + kind(ys)) * 2 + kind(xs))
        peers = []
        for a, b, k, e in hops:
            lt, ct = rem(long + a, 4), (c, 1 - c)[e]
            yt, pt = (ys, ys + 1 - 2 * rem(ys, 2))[b], (pair, pair + 1 - 2 * rem(pair, 2))[k]
            there = ((lt * 2 + rem(yt, 2)) * 2 + rem(pt, 2)) * 2 + ct
            zt, xt = (lt, pt) if h == 0 else (pt, lt)
            which = (kind(zt) * 2 + kind(yt)) * 2 + kind(xt)
            device = rem(zt + 4 - h, 4) * 32 + rem(yt + 4 - h, 4) * 8 + rem(xt + 4 - h, 4) * 2 + ct
            peers.append((device, there, which))
        group_peers.append(peers)
    chips = [z_at[dz] * 16 + y_at[dy] * 4 + x_at[dx] for dz, dy, dx in ALL]

    barrier = pltpu.get_barrier_semaphore()

    def greet(semaphore, device):
        pl.semaphore_signal(semaphore, inc=1, device_id=(device,), device_id_type=MESH)

    pairs = [
        (hidden_h, hidden), (again_h, again),
        (qw, wcat.at[:, pl.ds(0, 2048)]), (kw, wcat.at[:, pl.ds(2048, 512)]), (vw, wcat.at[:, pl.ds(2560, 512)]),
        (routing_h, routing), (rweight_h, rweight), (ow, obuf_s),
        (kc_h, kc), (vc_h, vc), (lengths_h, lengths), (lam_h, lam), (hgain_h, hgain), (mgain_h, mgain),
        (gate_h.at[0], gate), (up_h.at[0], up), (down_h.at[0], down), (sg_h, sg), (su_h, su), (sd_h, sd),
    ]
    copies = [pltpu.make_async_copy(src, dst, loc.at[i]) for i, (src, dst) in enumerate(pairs)]
    for copy in copies[:5]:
        copy.start()

    for i, (a, b, k, e) in enumerate(hops):
        greet(barrier, group_peers[0][i][0])
        if b:
            greet(barrier, group_peers[1][i][0])
    for zt in (z, 3 - z):
        for xt in (3 - x, 3 - (x + 1 - 2 * rem(x, 2))):
            for ct in (c, 1 - c):
                greet(barrier, zt * 32 + y * 8 + xt * 2 + ct)
    for copy in copies[5:]:
        copy.start()

    def ready(lo, hi):
        for copy in copies[lo:hi]:
            copy.wait()

    def remote(src, dst, phase, device):
        return pltpu.make_async_remote_copy(
            src_ref=src, dst_ref=dst, send_sem=snd.at[phase], recv_sem=rcv.at[phase],
            device_id=(device,), device_id_type=MESH,
        )

    def arrived(ref, phase):
        remote(ref, ref, phase, mate).wait_recv()

    def left(ref, phase):
        remote(ref, ref, phase, mate).wait_send()

    ready(0, 2)
    h32 = hidden[...].astype(F32)
    normed = rms(h32, again[...], 1e-6).astype(BF16).astype(F32)
    for i in range(2):
        for b in range(16):
            lines[i * 16 + b : i * 16 + b + 1, :] = normed[i : i + 1, b * 128 : b * 128 + 128]
    low = iota((1, 128), 1) < 64
    turned = [pltpu.roll(lines[...], 32 * i, 1) for i in (1, 2, 3)] + [lines[...]]
    for h in range(2):
        for which in range(8):
            sz, sy, sx = which // 4, which // 2 % 2, which % 2
            first_half, second_half = turned[h + 2 * sx], turned[(h + 2 - 2 * sx) % 4]
            for i in range(2):
                for zi in range(2):
                    zz = (((0, 3), (1, 2))[sz][zi] - h) % 4
                    left_at, right_at = (i * 16 + zz * 4 + (yy - h) % 4 for yy in ((0, 3), (1, 2))[sy])
                    line = jnp.where(low, first_half[left_at : left_at + 1], second_half[right_at : right_at + 1])
                    s1f[h, which, i * 2 + zi : i * 2 + zi + 1, :] = line
    s1[...] = s1f[...].astype(BF16)
    for j in range(16):
        hs[j] = h32[:, j * 128 : j * 128 + 128]
    ready(2, 5)
    pl.semaphore_wait(barrier, 55)

    for h in range(2):
        for device, there, which in group_peers[h]:
            remote(s1.at[h, which], r1.at[h, seat[h]], P1, device).start()
    for i in range(15):
        for h in range(2):
            device, col = cube_peers[h][i]
            remote(
                wcat.at[:, pl.ds(col, 384)], wbuf.at[h, pl.ds(cube_row[h], 16), :], W, device
            ).start()
    for device, there, which in group_peers[0]:
        greet(met, device)
    for h in range(2):
        wbuf[h, pl.ds(cube_row[h], 16), :] = wcat[:, pl.ds(cube_col[h], 384)]
        r1[h, seat[h]] = s1[h, my_kind[h]]
    hbuf[q] = hs[q]

    ready(5, 8)
    obuf[chip, c] = obuf_s[:, pl.ds(pl.multiple_of(q * 128, 128), 128)]
    sel = jnp.where(
        iota((128, 256), 1) == 4 * (iota((128, 256), 0) // 2) + 2 * c + iota((128, 256), 0) % 2, 1.0, 0.0
    ).astype(BF16)
    before = jnp.where(iota((256, 256), 0) < iota((256, 256), 1), 1.0, 0.0).astype(BF16)
    picks, back, slot_weight = [], [], []
    for i, expert in enumerate((me, mate)):
        hit = routing[...] == expert
        here = jnp.sum(jnp.where(hit, 1.0, 0.0), axis=0, keepdims=True)
        rank = dot(jnp.broadcast_to(here, (16, 256)).astype(BF16), before)[0:1]
        full = jnp.where(rank == iota((SLOTS, 256), 0).astype(F32), here, 0.0)
        back.append(dot_nt(sel, full.astype(BF16)))
        weight = jnp.sum(jnp.where(hit, rweight[...], 0.0), axis=0, keepdims=True)
        slot_weight.append(jnp.sum(full * weight, axis=1, keepdims=True))
        mark = (iota((SLOTS, 256), 0) - OWN == iota((SLOTS, 256), 1) - 2 * expert) & (
            iota((SLOTS, 256), 1) // 2 == expert
        )
        full = full + jnp.where(mark, 1.0, 0.0)
        picks.append(dot_nt(full.astype(BF16), sel))
    picks = jnp.concatenate(picks, axis=0).astype(BF16)
    back = jnp.concatenate(back, axis=1).astype(BF16)

    arrived(r1.at[:, pl.ds(0, 31)], P1)
    for h in range(2):
        for i in range(32):
            x1[h, 4 * i : 4 * i + 4, :] = r1[h, i].astype(F32)
    arrived(wbuf.at[:, pl.ds(0, 240), :], W)
    for h in range(2):
        wide = jnp.concatenate([x1[h, pl.ds(b, 64, stride=2), :].astype(BF16) for b in range(2)], axis=1)
        part[h] = dot(wide, wbuf[h])
        for i in range(32):
            s2[h, i] = part[h, 2 * i : 2 * i + 2, :]

    for i in range(31):
        for h in range(2):
            device, there, which = group_peers[h][i]
            remote(s2.at[h, there], r2.at[h, seat[h]], P2, device).start()
    for h in range(2):
        r2[h, seat[h]] = s2[h, seat[h]]
    pl.semaphore_wait(met, 31)
    for t in chips:
        col = pl.multiple_of(rem(t, 16) * 128, 128)
        remote(obuf_s.at[:, pl.ds(col, 128)], obuf.at[chip, c], O, t * 2 + c).start()
    for dy, dx in NEAR[:-1]:
        t = y_at[dy] * 4 + x_at[dx]
        remote(hs.at[t], hbuf.at[q], HID, z * 32 + t * 2 + c).start()
    ready(14, 17)
    remote(gate, gate_x, GX, mate).start()
    remote(up, up_x, UX, mate).start()
    arrived(r2.at[:, pl.ds(0, 31)], P2)

    for u in range(24):
        at = (u % 3) * 128
        val = None
        for src in range(32):
            if (src // 16) * 2 + src % 2 == u // 3 % 4:
                term = r2[u // 12, src, :, at : at + 128]
                val = term if val is None else val + term
        for s in range(2):
            line = val[s : s + 1, :]
            if u < 16:
                r = (u % 2) * 8 + u // 2
                qscr[s, r : r + 1, :] = line
            elif u < 20:
                kscr[s, u - 16 : u - 15, :] = line
            else:
                v = u - 20
                vscr[s, v // 2 : v // 2 + 1, (v % 2) * 128 : (v % 2) * 128 + 128] = line

    ready(8, 14)
    rows = iota((16, 1), 0)
    pair_of = (rows // 8) + 2 * ((rows % 8) // 4)
    first = iota((8, 1), 0) < 4
    lam_col = jnp.sum(jnp.where(iota((8, 8), 0) == iota((8, 8), 1), lam[...], 0.0), axis=1, keepdims=True)
    scale = 128 ** (-0.5)
    place = iota((1, CACHE), 1)
    lane = iota((1, 128), 1)
    inverse = jnp.exp((lane % 64).astype(F32) * (-13.122363377404328 / 64))

    def turn(v, cos_row, sin_row):
        return (v * cos_row + pltpu.roll(v, 64, 1) * sin_row).astype(BF16)

    q_rows, k_rows, v_rows, all_scores = [], [], [], []
    for s in range(2):
        angle = lengths[s].astype(F32) * inverse
        cos_row = jnp.cos(angle)
        sin_row = jnp.sin(angle)
        sin_row = jnp.where(lane < 64, -sin_row, sin_row)
        qq = turn(qscr[s], cos_row, sin_row).astype(F32)
        wide = jnp.concatenate([jnp.where(pair_of == u, qq, 0.0) for u in range(4)], axis=1).astype(BF16)
        all_scores.append(dot_nt(wide, kc[s]))
        kn = turn(kscr[s], cos_row, sin_row)
        vn = vscr[s].astype(BF16)
        for u in range(4):
            out[s : s + 1, D + u * 128 : D + u * 128 + 128] = kn[u : u + 1]
        for u in range(2):
            out[s : s + 1, D + 512 + u * 256 : D + 512 + u * 256 + 256] = vn[u : u + 1]
        q_rows.append(qq)
        k_rows.append(kn.astype(F32))
        v_rows.append(vn.astype(F32))
    sums, own_parts = [], []
    for s in range(2):
        qq, kn = q_rows[s], k_rows[s]
        scores = all_scores[s] * scale
        k_of = jnp.where(
            pair_of == 0, kn[0:1], jnp.where(pair_of == 1, kn[1:2], jnp.where(pair_of == 2, kn[2:3], kn[3:4]))
        )
        own_score = jnp.sum(qq * k_of, axis=1, keepdims=True) * scale
        live = place < lengths[s]
        peak = jnp.maximum(jnp.max(jnp.where(live, scores, -jnp.inf), axis=1, keepdims=True), own_score)
        weights = jnp.where(live, jnp.exp(scores - peak), 0.0)
        own_weight = jnp.exp(own_score - peak)
        share = 1.0 / (jnp.sum(weights, axis=1, keepdims=True) + own_weight)
        maps = weights * share
        own_maps = own_weight * share
        combined = (maps[:8] - lam_col * maps[8:]).astype(BF16)
        own_parts.append((own_maps[:8] - lam_col * own_maps[8:]).astype(BF16).astype(F32))
        sums.append(dot(combined, vc[s]))
    for s in range(2):
        head_out = jnp.where(first, sums[s][:, :256], sums[s][:, 256:])
        head_out = head_out + own_parts[s] * jnp.where(first, v_rows[s][0:1], v_rows[s][1:2])
        att = rms(head_out, hgain[...], 1e-5)
        for h in range(8):
            for half in range(2):
                at16[s, 2 * h + half : 2 * h + half + 1, :] = att[h : h + 1, half * 128 : half * 128 + 128]
        s3[s] = at16[s].astype(BF16)

    for dy, dx in NEAR[:-1]:
        t = y_at[dy] * 4 + x_at[dx]
        remote(s3, r3.at[q], P3, z * 32 + t * 2 + c).start()
    r3[q] = s3[...]
    arrived(obuf.at[pl.ds(0, 63), 0], O)
    remote(obuf.at[:, c], obuf.at[:, c], OX, mate).start()
    remote(down, down_x, DX, mate).start()
    arrived(hbuf.at[pl.ds(0, 15)], HID)
    for i in range(16):
        hb[2 * i : 2 * i + 2, :] = hbuf[i]
    arrived(obuf.at[:, 0], OX)
    arrived(r3.at[pl.ds(0, 15)], P3)
    x3[...] = r3[...].reshape(512, 128).astype(F32)
    wide = jnp.concatenate([x3[pl.ds(b, 32, stride=16), :].astype(BF16) for b in range(16)], axis=1)
    proj = dot(wide, obuf[...].reshape(D, 128))
    mixed = (hb[...] + proj.astype(BF16).astype(F32)).astype(BF16)
    am[...] = mixed
    gat[q, z] = mixed

    for t in chips:
        remote(am, gat.at[q, z], P5, t * 2 + c).start()
    ready(17, 20)
    arrived(racc.at[pl.ds(0, CHIPS - 1)], P5)
    for b in range(8):
        cols = jnp.concatenate([gat[2 * b].reshape(128, 128), gat[2 * b + 1].reshape(128, 128)], axis=1)
        mine[:, b * 256 : b * 256 + 256] = dot(picks, cols)
    arrived(gate_x, GX)
    arrived(up_x, UX)
    arrived(down_x, DX)
    mixed = mine[...]
    moe = rms(mixed, mgain[...], 1e-6).astype(BF16)
    for i, (g, u, d) in enumerate(((gate, up, down), (gate_x, up_x, down_x))):
        rows = moe[i * SLOTS : i * SLOTS + SLOTS]
        hid = (jax.nn.silu(dot(rows, g[...])) * dot(rows, u[...])).astype(BF16)
        answer = dot(hid, d[...]).astype(BF16).astype(F32) * slot_weight[i]
        for b in range(8):
            ans[b, i * SLOTS : i * SLOTS + SLOTS] = answer[:, b * 256 : b * 256 + 256].astype(BF16)
    for b in range(8):
        tiles = dot(back, ans[b])
        for half in range(2):
            spread[half, pl.ds(b, 128, stride=8), :] = tiles[:, half * 128 : half * 128 + 128]
    for k in (2, 1, 3, 0):
        owners = pl.ds(pl.multiple_of(z_at[k] * 16, 16), 16)
        rows = pl.ds(pl.multiple_of(z_at[k] * 256, 256), 256)
        tiles = jnp.concatenate([spread[0, rows, :], spread[1, rows, :]], axis=1)
        res[owners] = tiles.astype(BF16).reshape(16, 16, 256)
        for dy, dx in NEAR if k else NEAR[:-1]:
            t = z_at[k] * 16 + y_at[dy] * 4 + x_at[dx]
            remote(res.at[t], racc.at[chip], P6, t * 2 + c).start()
    racc[chip] = res[chip]
    moe = moe[:SLOTS]
    hid = (jax.nn.silu(dot(moe, sg[...])) * dot(moe, su[...])).astype(BF16)
    shared = dot(hid[OWN:], sd[...])
    left(wbuf.at[:, pl.ds(0, 240), :], W)
    left(obuf.at[pl.ds(0, 63), 0], O)
    left(obuf.at[:, 0], OX)
    left(hbuf.at[pl.ds(0, 15)], HID)
    left(r1.at[:, pl.ds(0, 31)], P1)
    left(r2.at[:, pl.ds(0, 31)], P2)
    left(r3.at[pl.ds(0, 15)], P3)
    left(racc.at[pl.ds(0, CHIPS - 1)], P5)
    left(gate, GX)
    left(up, UX)
    left(down, DX)
    arrived(racc.at[pl.ds(0, CHIPS - 1)], P6)

    def add(i, carry):
        return carry + racc[i].astype(F32)

    total = lax.fori_loop(0, CHIPS, add, jnp.zeros((16, 256), F32), unroll=8)
    for s in range(2):
        for b in range(8):
            fin[s : s + 1, b * 256 : b * 256 + 256] = total[s * 8 + b : s * 8 + b + 1]
    out[:, 0:D] = (mixed[OWN : OWN + 2] + fin[...] + shared[0:2]).astype(BF16)
    left(racc.at[pl.ds(0, CHIPS - 1)], P6)


def on_device(
    hidden_in, lengths, key_cache, value_cache, query_w, key_w, value_w, out_w, lam_heads, head_gain,
    attn_gain, moe_gain, routing, route_weight, gate_w, up_w, down_w, shared_gate, shared_up, shared_down,
):
    hbm = pl.BlockSpec(memory_space=pl.ANY)
    scratch = [
        ((2, D), BF16), ((1, 8), F32), ((1, 256), F32), ((1, D), F32), ((1, D), F32),
        ((6, 256), jnp.int32), ((6, 256), F32),
        ((16, 3072), BF16), ((16, D), BF16), ((2, 256, 384), BF16), ((CHIPS, 2, 16, 128), BF16),
        ((2, CACHE, 512), BF16), ((2, CACHE, 512), BF16),
        ((D, 512), BF16), ((D, 512), BF16), ((512, D), BF16),
        ((D, 512), BF16), ((D, 512), BF16), ((512, D), BF16),
        ((D, 512), BF16), ((D, 512), BF16), ((512, D), BF16),
        ((16, 2, 128), F32), ((16, 2, 128), F32), ((32, 128), F32),
        ((32, 128), F32), ((2, 8, 4, 128), F32), ((2, 8, 4, 128), BF16), ((2, 32, 4, 128), BF16), ((2, 128, 128), F32), ((2, 64, 384), F32),
        ((2, 32, 2, 384), F32), ((2, 32, 2, 384), F32),
        ((2, 16, 128), F32), ((2, 4, 128), F32), ((2, 2, 256), F32),
        ((2, 16, 128), F32), ((2, 16, 128), BF16), ((16, 2, 16, 128), BF16), ((512, 128), F32),
        ((32, 128), BF16), ((16, 4, 32, 128), BF16), ((2, 1024, 128), F32),
        ((2 * SLOTS, D), F32),
        ((8, 2 * SLOTS, 256), BF16), ((CHIPS, 16, 256), BF16), ((CHIPS, 16, 256), BF16), ((2, D), F32),
    ]
    packed = pl.pallas_call(
        kernel,
        out_shape=jax.ShapeDtypeStruct((2, D + 1024), BF16),
        in_specs=[hbm] * 20,
        out_specs=pl.BlockSpec(memory_space=pltpu.VMEM),
        scratch_shapes=[pltpu.SMEM((2,), jnp.int32)]
        + [pltpu.VMEM(*s) for s in scratch]
        + [pltpu.SemaphoreType.DMA((20,)), pltpu.SemaphoreType.DMA((12,)), pltpu.SemaphoreType.DMA((12,))]
        + [pltpu.SemaphoreType.REGULAR],
        compiler_params=pltpu.CompilerParams(
            collective_id=0, has_side_effects=True, vmem_limit_bytes=60 * 1024 * 1024
        ),
    )(
        lengths, hidden_in, lam_heads.reshape(1, 8), head_gain.reshape(1, 256),
        attn_gain.reshape(1, D), moe_gain.reshape(1, D), routing.T, route_weight.T,
        query_w, key_w, value_w, out_w, key_cache, value_cache, gate_w, up_w, down_w,
        shared_gate, shared_up, shared_down,
    )

    def unpack(src, layer, key, value):
        layer[...] = src[:, 0:D]
        key[...] = src[:, D : D + 512]
        value[...] = src[:, D + 512 :]

    vmem = pl.BlockSpec(memory_space=pltpu.VMEM)
    return pl.pallas_call(
        unpack,
        out_shape=(
            jax.ShapeDtypeStruct((2, D), BF16),
            jax.ShapeDtypeStruct((2, 512), BF16),
            jax.ShapeDtypeStruct((2, 512), BF16),
        ),
        in_specs=[vmem],
        out_specs=(vmem, vmem, vmem),
        compiler_params=pltpu.CompilerParams(vmem_limit_bytes=60 * 1024 * 1024),
    )(packed)


def solution(mesh):
    e2, e3 = P("ep", None), P("ep", None, None)
    return jax.shard_map(
        on_device,
        mesh=mesh,
        in_specs=(
            e2, P("ep"), e3, e3, e2, e2, e2, e2, P(), P(), P(), P(), P(), P(), e3, e3, e3, P(), P(), P(),
        ),
        out_specs=(e2, e2, e2),
        check_vma=False,
    )
```

```python
import jax
import jax.numpy as jnp
from jax import lax
from jax.experimental import pallas as pl
from jax.experimental.pallas import tpu as pltpu
from jax.sharding import PartitionSpec as P

F32 = jnp.float32
BF16 = jnp.bfloat16
MESH = pl.DeviceIdType.MESH
N = 128
CHIPS = 64
D = 2048
CACHE = 1024
SLOTS = 32
OWN = 24
W, O, OX, HID, P1, P2, P3, GX, UX, DX, P6, P5 = range(12)


def dot(a, b):
    return jnp.dot(a, b, preferred_element_type=F32)


def dot_nt(a, b):
    return lax.dot_general(a, b, (((1,), (1,)), ((), ())), preferred_element_type=F32)


def rem(a, b):
    return lax.rem(a, jnp.int32(b))


def div(a, b):
    return lax.div(a, jnp.int32(b))


def kind(v):
    return rem(div(v + 1, 2), 2)


def far(pair):
    return -sum(min(k, 4 - k) for k in pair)


NEAR = sorted(((a, b) for a in range(4) for b in range(4)), key=far)
ALL = sorted(((a, b, k) for a in range(4) for b in range(4) for k in range(4)), key=far)[:-1]


def iota(shape, dim):
    return lax.broadcasted_iota(jnp.int32, shape, dim)


def rms(x, gain, eps):
    return x * lax.rsqrt(jnp.mean(x * x, axis=-1, keepdims=True) + eps) * gain


def kernel(
    lengths_h, hidden_h, lam_h, hgain_h, again_h, mgain_h, routing_h, rweight_h,
    qw, kw, vw, ow, kc_h, vc_h, gate_h, up_h, down_h, sg_h, su_h, sd_h,
    out,
    lengths, hidden, lam, hgain, again, mgain, routing, rweight,
    wcat, obuf_s, wbuf, obuf, kc, vc, gate, up, down, gate_x, up_x, down_x, sg, su, sd,
    hs, hbuf, hb, lines, s1f, s1, r1, x1, part, s2, r2, angles, qscr, kscr, vscr, at16, s3, r3, x3,
    am, gat, spread, mine, pre, ans, res, racc, fin,
    loc, snd, rcv, met,
):
    me = lax.axis_index("ep")
    z = div(me, 32)
    y = rem(div(me, 8), 4)
    xc = rem(me, 8)
    c = rem(me, 2)
    chip = div(me, 2)
    q = rem(chip, 16)
    mate = me + 1 - 2 * c

    x = div(xc, 2)
    z_at = [rem(z + k, 4) for k in range(4)]
    y_at = [rem(y + k, 4) for k in range(4)]
    x_at = [rem(x + k, 4) for k in range(4)]
    flips = sorted(((a, b, k, e) for a in (0, 1) for b in (0, 1) for k in (0, 1) for e in (0, 1)), key=sum)[:0:-1]
    hops = sorted(
        ((a, b, k, e) for a in range(4) for b in (0, 1) for k in (0, 1) for e in (0, 1)),
        key=lambda h: -(min(h[0], 4 - h[0]) + h[1] + h[2] + 0.1 * h[3]),
    )[:-1]
    cube_peers, cube_row, cube_col, group_peers, seat, my_kind = [], [], [], [], [], []
    for h in range(2):
        zs, ys, xs = (rem(v + h, 4) for v in (z, y, x))
        zo, yo, xo = (rem(7 - v - h, 4) for v in (zs, ys, xs))
        long, pair = (zs, xs) if h == 0 else (xs, zs)
        peers = []
        for a, b, k, e in flips:
            zt, yt, xt, ct = (z, zo)[a], (y, yo)[b], (x, xo)[k], (c, 1 - c)[e]
            lt = rem((zt, xt)[h] + h, 4)
            col = pl.multiple_of(h * 1536 + (div(lt, 2) * 2 + ct) * 384, 128)
            peers.append((zt * 32 + yt * 8 + xt * 2 + ct, col))
        cube_peers.append(peers)
        at = div(zs, 2) * 128 + div(ys, 2) * 64 + c * 16
        cube_row.append(pl.multiple_of(at + 32 * jnp.where(kind(xs) == 1, div(xs, 2), 1 - div(xs, 2)), 16))
        cube_col.append(pl.multiple_of(h * 1536 + (div(long, 2) * 2 + c) * 384, 128))
        seat.append(((long * 2 + rem(ys, 2)) * 2 + rem(pair, 2)) * 2 + c)
        my_kind.append((kind(zs) * 2 + kind(ys)) * 2 + kind(xs))
        peers = []
        for a, b, k, e in hops:
            lt, ct = rem(long + a, 4), (c, 1 - c)[e]
            yt, pt = (ys, ys + 1 - 2 * rem(ys, 2))[b], (pair, pair + 1 - 2 * rem(pair, 2))[k]
            there = ((lt * 2 + rem(yt, 2)) * 2 + rem(pt, 2)) * 2 + ct
            zt, xt = (lt, pt) if h == 0 else (pt, lt)
            which = (kind(zt) * 2 + kind(yt)) * 2 + kind(xt)
            device = rem(zt + 4 - h, 4) * 32 + rem(yt + 4 - h, 4) * 8 + rem(xt + 4 - h, 4) * 2 + ct
            peers.append((device, there, which))
        group_peers.append(peers)
    chips = [z_at[dz] * 16 + y_at[dy] * 4 + x_at[dx] for dz, dy, dx in ALL]

    barrier = pltpu.get_barrier_semaphore()

    def greet(semaphore, device):
        pl.semaphore_signal(semaphore, inc=1, device_id=(device,), device_id_type=MESH)

    pairs = [
        (hidden_h, hidden), (again_h, again),
        (qw, wcat.at[:, pl.ds(0, 2048)]), (kw, wcat.at[:, pl.ds(2048, 512)]), (vw, wcat.at[:, pl.ds(2560, 512)]),
        (routing_h, routing), (rweight_h, rweight), (ow, obuf_s),
        (kc_h, kc), (vc_h, vc), (lengths_h, lengths), (lam_h, lam), (hgain_h, hgain), (mgain_h, mgain),
        (gate_h.at[0], gate), (up_h.at[0], up), (down_h.at[0], down), (sg_h, sg), (su_h, su), (sd_h, sd),
    ]
    copies = [pltpu.make_async_copy(src, dst, loc.at[i]) for i, (src, dst) in enumerate(pairs)]
    for copy in copies[:5]:
        copy.start()

    for i, (a, b, k, e) in enumerate(hops):
        greet(barrier, group_peers[0][i][0])
        if b:
            greet(barrier, group_peers[1][i][0])
    for zt in (z, 3 - z):
        for xt in (3 - x, 3 - (x + 1 - 2 * rem(x, 2))):
            for ct in (c, 1 - c):
                greet(barrier, zt * 32 + y * 8 + xt * 2 + ct)
    for copy in copies[5:]:
        copy.start()

    def ready(lo, hi):
        for copy in copies[lo:hi]:
            copy.wait()

    def remote(src, dst, phase, device):
        return pltpu.make_async_remote_copy(
            src_ref=src, dst_ref=dst, send_sem=snd.at[phase], recv_sem=rcv.at[phase],
            device_id=(device,), device_id_type=MESH,
        )

    def arrived(ref, phase):
        remote(ref, ref, phase, mate).wait_recv()

    def left(ref, phase):
        remote(ref, ref, phase, mate).wait_send()

    ready(0, 2)
    h32 = hidden[...].astype(F32)
    normed = rms(h32, again[...], 1e-6).astype(BF16).astype(F32)
    for i in range(2):
        for b in range(16):
            lines[i * 16 + b : i * 16 + b + 1, :] = normed[i : i + 1, b * 128 : b * 128 + 128]
    low = iota((1, 128), 1) < 64
    turned = [pltpu.roll(lines[...], 32 * i, 1) for i in (1, 2, 3)] + [lines[...]]
    for h in range(2):
        for which in range(8):
            sz, sy, sx = which // 4, which // 2 % 2, which % 2
            first_half, second_half = turned[h + 2 * sx], turned[(h + 2 - 2 * sx) % 4]
            for i in range(2):
                for zi in range(2):
                    zz = (((0, 3), (1, 2))[sz][zi] - h) % 4
                    left_at, right_at = (i * 16 + zz * 4 + (yy - h) % 4 for yy in ((0, 3), (1, 2))[sy])
                    line = jnp.where(low, first_half[left_at : left_at + 1], second_half[right_at : right_at + 1])
                    s1f[h, which, i * 2 + zi : i * 2 + zi + 1, :] = line
    s1[...] = s1f[...].astype(BF16)
    for j in range(16):
        hs[j] = h32[:, j * 128 : j * 128 + 128]
    ready(2, 5)
    pl.semaphore_wait(barrier, 55)

    for h in range(2):
        for device, there, which in group_peers[h]:
            remote(s1.at[h, which], r1.at[h, seat[h]], P1, device).start()
    for i in range(15):
        for h in range(2):
            device, col = cube_peers[h][i]
            remote(
                wcat.at[:, pl.ds(col, 384)], wbuf.at[h, pl.ds(cube_row[h], 16), :], W, device
            ).start()
    for device, there, which in group_peers[0]:
        greet(met, device)
    for h in range(2):
        wbuf[h, pl.ds(cube_row[h], 16), :] = wcat[:, pl.ds(cube_col[h], 384)]
        r1[h, seat[h]] = s1[h, my_kind[h]]
    hbuf[q] = hs[q]

    ready(5, 8)
    obuf[chip, c] = obuf_s[:, pl.ds(pl.multiple_of(q * 128, 128), 128)]
    sel = jnp.where(
        iota((128, 256), 1) == 4 * (iota((128, 256), 0) // 2) + 2 * c + iota((128, 256), 0) % 2, 1.0, 0.0
    ).astype(BF16)
    before = jnp.where(iota((256, 256), 0) < iota((256, 256), 1), 1.0, 0.0).astype(BF16)
    picks, back, slot_weight = [], [], []
    for i, expert in enumerate((me, mate)):
        hit = routing[...] == expert
        here = jnp.sum(jnp.where(hit, 1.0, 0.0), axis=0, keepdims=True)
        rank = dot(jnp.broadcast_to(here, (16, 256)).astype(BF16), before)[0:1]
        full = jnp.where(rank == iota((SLOTS, 256), 0).astype(F32), here, 0.0)
        back.append(dot_nt(sel, full.astype(BF16)))
        weight = jnp.sum(jnp.where(hit, rweight[...], 0.0), axis=0, keepdims=True)
        slot_weight.append(jnp.sum(full * weight, axis=1, keepdims=True))
        mark = (iota((SLOTS, 256), 0) - OWN == iota((SLOTS, 256), 1) - 2 * expert) & (
            iota((SLOTS, 256), 1) // 2 == expert
        )
        full = full + jnp.where(mark, 1.0, 0.0)
        picks.append(dot_nt(full.astype(BF16), sel))
    picks = jnp.concatenate(picks, axis=0).astype(BF16)
    back = jnp.concatenate(back, axis=1).astype(BF16)

    ready(8, 14)
    lane = iota((1, 128), 1)
    inverse = jnp.exp((lane % 64).astype(F32) * (-13.122363377404328 / 64))
    for s in range(2):
        angle = lengths[s].astype(F32) * inverse
        angles[0, s : s + 1, :] = jnp.cos(angle)
        angles[1, s : s + 1, :] = jnp.where(lane < 64, -jnp.sin(angle), jnp.sin(angle))

    arrived(r1.at[:, pl.ds(0, 31)], P1)
    for h in range(2):
        for i in range(32):
            x1[h, 4 * i : 4 * i + 4, :] = r1[h, i].astype(F32)
    arrived(wbuf.at[:, pl.ds(0, 240), :], W)
    for h in range(2):
        wide = jnp.concatenate([x1[h, pl.ds(b, 64, stride=2), :].astype(BF16) for b in range(2)], axis=1)
        part[h] = dot(wide, wbuf[h])
        for i in range(32):
            s2[h, i] = part[h, 2 * i : 2 * i + 2, :]

    for i in range(31):
        for h in range(2):
            device, there, which = group_peers[h][i]
            remote(s2.at[h, there], r2.at[h, seat[h]], P2, device).start()
    for h in range(2):
        r2[h, seat[h]] = s2[h, seat[h]]
    pl.semaphore_wait(met, 31)
    for t in chips:
        col = pl.multiple_of(rem(t, 16) * 128, 128)
        remote(obuf_s.at[:, pl.ds(col, 128)], obuf.at[chip, c], O, t * 2 + c).start()
    for dy, dx in NEAR[:-1]:
        t = y_at[dy] * 4 + x_at[dx]
        remote(hs.at[t], hbuf.at[q], HID, z * 32 + t * 2 + c).start()
    ready(14, 17)
    remote(gate, gate_x, GX, mate).start()
    remote(up, up_x, UX, mate).start()
    arrived(r2.at[:, pl.ds(0, 31)], P2)

    for u in range(24):
        at = (u % 3) * 128
        val = None
        for src in range(32):
            if (src // 16) * 2 + src % 2 == u // 3 % 4:
                term = r2[u // 12, src, :, at : at + 128]
                val = term if val is None else val + term
        for s in range(2):
            line = val[s : s + 1, :]
            if u < 16:
                r = (u % 2) * 8 + u // 2
                qscr[s, r : r + 1, :] = line
            elif u < 20:
                kscr[s, u - 16 : u - 15, :] = line
            else:
                v = u - 20
                vscr[s, v // 2 : v // 2 + 1, (v % 2) * 128 : (v % 2) * 128 + 128] = line

    rows = iota((16, 1), 0)
    pair_of = (rows // 8) + 2 * ((rows % 8) // 4)
    first = iota((8, 1), 0) < 4
    lam_col = jnp.sum(jnp.where(iota((8, 8), 0) == iota((8, 8), 1), lam[...], 0.0), axis=1, keepdims=True)
    scale = 128 ** (-0.5)

    def turn(v, cos_row, sin_row):
        return (v * cos_row + pltpu.roll(v, 64, 1) * sin_row).astype(BF16)

    q_rows, k_rows, v_rows, all_scores = [], [], [], []
    for s in range(2):
        cos_row, sin_row = angles[0, s : s + 1, :], angles[1, s : s + 1, :]
        qq = turn(qscr[s], cos_row, sin_row).astype(F32)
        wide = jnp.concatenate([jnp.where(pair_of == u, qq, 0.0) for u in range(4)], axis=1).astype(BF16)
        all_scores.append(dot_nt(wide, kc[s]))
        kn = turn(kscr[s], cos_row, sin_row)
        vn = vscr[s].astype(BF16)
        for u in range(4):
            out[s : s + 1, D + u * 128 : D + u * 128 + 128] = kn[u : u + 1]
        for u in range(2):
            out[s : s + 1, D + 512 + u * 256 : D + 512 + u * 256 + 256] = vn[u : u + 1]
        q_rows.append(qq)
        k_rows.append(kn.astype(F32))
        v_rows.append(vn.astype(F32))
    sums, own_parts = [], []
    for s in range(2):
        qq, kn = q_rows[s], k_rows[s]
        scores = all_scores[s] * scale
        k_of = jnp.where(
            pair_of == 0, kn[0:1], jnp.where(pair_of == 1, kn[1:2], jnp.where(pair_of == 2, kn[2:3], kn[3:4]))
        )
        own_score = jnp.sum(qq * k_of, axis=1, keepdims=True) * scale
        live = iota((1, CACHE), 1) < lengths[s]
        peak = jnp.maximum(jnp.max(jnp.where(live, scores, -jnp.inf), axis=1, keepdims=True), own_score)
        weights = jnp.where(live, jnp.exp(scores - peak), 0.0)
        own_weight = jnp.exp(own_score - peak)
        share = 1.0 / (jnp.sum(weights, axis=1, keepdims=True) + own_weight)
        maps = weights * share
        own_maps = own_weight * share
        combined = (maps[:8] - lam_col * maps[8:]).astype(BF16)
        own_parts.append((own_maps[:8] - lam_col * own_maps[8:]).astype(BF16).astype(F32))
        sums.append(dot(combined, vc[s]))
    for s in range(2):
        head_out = jnp.where(first, sums[s][:, :256], sums[s][:, 256:])
        head_out = head_out + own_parts[s] * jnp.where(first, v_rows[s][0:1], v_rows[s][1:2])
        att = rms(head_out, hgain[...], 1e-5)
        for h in range(8):
            for half in range(2):
                at16[s, 2 * h + half : 2 * h + half + 1, :] = att[h : h + 1, half * 128 : half * 128 + 128]
        s3[s] = at16[s].astype(BF16)

    for dy, dx in NEAR[:-1]:
        t = y_at[dy] * 4 + x_at[dx]
        remote(s3, r3.at[q], P3, z * 32 + t * 2 + c).start()
    r3[q] = s3[...]
    arrived(obuf.at[pl.ds(0, 63), 0], O)
    remote(obuf.at[:, c], obuf.at[:, c], OX, mate).start()
    remote(down, down_x, DX, mate).start()
    arrived(hbuf.at[pl.ds(0, 15)], HID)
    for i in range(16):
        hb[2 * i : 2 * i + 2, :] = hbuf[i]
    arrived(obuf.at[:, 0], OX)
    arrived(r3.at[pl.ds(0, 15)], P3)
    x3[...] = r3[...].reshape(512, 128).astype(F32)
    wide = jnp.concatenate([x3[pl.ds(b, 32, stride=16), :].astype(BF16) for b in range(16)], axis=1)
    proj = dot(wide, obuf[...].reshape(D, 128))
    mixed = (hb[...] + proj.astype(BF16).astype(F32)).astype(BF16)
    am[...] = mixed
    gat[q, z] = mixed

    for dy in (2, 1, 3, 0):
        for dz, dx in NEAR if dy else NEAR[:-1]:
            t = z_at[dz] * 16 + y_at[dy] * 4 + x_at[dx]
            remote(am, gat.at[q, z], P5 + dy, t * 2 + c).start()
    ready(17, 20)
    squares = jnp.zeros((2 * SLOTS, 1), F32)
    for k, dy in enumerate((2, 1, 3, 0)):
        arrived(racc.at[pl.ds(0, 16 if dy else 15)], P5 + dy)
        if k == 0:
            arrived(gate_x, GX)
            arrived(up_x, UX)
            arrived(down_x, DX)
        ys = y_at[4 - dy if dy else 0]
        at = pl.multiple_of(ys * 512, 512)
        tiles = [gat[ys * 4 + i].reshape(128, 128) for i in range(4)]
        got = jnp.concatenate(
            [dot(picks, jnp.concatenate(tiles[i : i + 2], axis=1)) for i in (0, 2)], axis=1
        )
        mine[:, pl.ds(at, 512)] = got[OWN:SLOTS]
        squares = squares + jnp.sum(got * got, axis=1, keepdims=True)
        got = (got * mgain[:, pl.ds(at, 512)]).astype(BF16)
        for i, (g, u) in enumerate(((gate, up), (gate_x, up_x))):
            rows = got[i * SLOTS : i * SLOTS + SLOTS]
            for j, w in enumerate((g, u)):
                term = dot(rows, w[pl.ds(at, 512), :])
                pre[i, j] = term if k == 0 else pre[i, j] + term
    factor = lax.rsqrt(squares / D + 1e-6)
    for i, d in enumerate((down, down_x)):
        f = factor[i * SLOTS : i * SLOTS + SLOTS]
        hid = (jax.nn.silu(pre[i, 0] * f) * (pre[i, 1] * f)).astype(BF16)
        answer = dot(hid, d[...]).astype(BF16).astype(F32) * slot_weight[i]
        for b in range(8):
            ans[b, i * SLOTS : i * SLOTS + SLOTS] = answer[:, b * 256 : b * 256 + 256].astype(BF16)
    for b in range(8):
        tiles = dot(back, ans[b])
        for half in range(2):
            spread[half, pl.ds(b, 128, stride=8), :] = tiles[:, half * 128 : half * 128 + 128]
    for k in (2, 1, 3, 0):
        owners = pl.ds(pl.multiple_of(z_at[k] * 16, 16), 16)
        rows = pl.ds(pl.multiple_of(z_at[k] * 256, 256), 256)
        tiles = jnp.concatenate([spread[0, rows, :], spread[1, rows, :]], axis=1)
        res[owners] = tiles.astype(BF16).reshape(16, 16, 256)
        for dy, dx in NEAR if k else NEAR[:-1]:
            t = z_at[k] * 16 + y_at[dy] * 4 + x_at[dx]
            remote(res.at[t], racc.at[chip], P6, t * 2 + c).start()
    racc[chip] = res[chip]
    mixed = mine[...]
    moe = rms(mixed, mgain[...], 1e-6).astype(BF16)
    hid = (jax.nn.silu(dot(moe, sg[...])) * dot(moe, su[...])).astype(BF16)
    shared = dot(hid, sd[...])
    left(wbuf.at[:, pl.ds(0, 240), :], W)
    left(obuf.at[pl.ds(0, 63), 0], O)
    left(obuf.at[:, 0], OX)
    left(hbuf.at[pl.ds(0, 15)], HID)
    left(r1.at[:, pl.ds(0, 31)], P1)
    left(r2.at[:, pl.ds(0, 31)], P2)
    left(r3.at[pl.ds(0, 15)], P3)
    for dy in range(4):
        left(racc.at[pl.ds(0, 16 if dy else 15)], P5 + dy)
    left(gate, GX)
    left(up, UX)
    left(down, DX)
    arrived(racc.at[pl.ds(0, CHIPS - 1)], P6)

    def add(i, carry):
        return carry + racc[i].astype(F32)

    total = lax.fori_loop(0, CHIPS, add, jnp.zeros((16, 256), F32), unroll=8)
    for s in range(2):
        for b in range(8):
            fin[s : s + 1, b * 256 : b * 256 + 256] = total[s * 8 + b : s * 8 + b + 1]
    out[:, 0:D] = (mixed[0:2] + fin[...] + shared[0:2]).astype(BF16)
    left(racc.at[pl.ds(0, CHIPS - 1)], P6)


def on_device(
    hidden_in, lengths, key_cache, value_cache, query_w, key_w, value_w, out_w, lam_heads, head_gain,
    attn_gain, moe_gain, routing, route_weight, gate_w, up_w, down_w, shared_gate, shared_up, shared_down,
):
    hbm = pl.BlockSpec(memory_space=pl.ANY)
    scratch = [
        ((2, D), BF16), ((1, 8), F32), ((1, 256), F32), ((1, D), F32), ((1, D), F32),
        ((6, 256), jnp.int32), ((6, 256), F32),
        ((16, 3072), BF16), ((16, D), BF16), ((2, 256, 384), BF16), ((CHIPS, 2, 16, 128), BF16),
        ((2, CACHE, 512), BF16), ((2, CACHE, 512), BF16),
        ((D, 512), BF16), ((D, 512), BF16), ((512, D), BF16),
        ((D, 512), BF16), ((D, 512), BF16), ((512, D), BF16),
        ((D, 512), BF16), ((D, 512), BF16), ((512, D), BF16),
        ((16, 2, 128), F32), ((16, 2, 128), F32), ((32, 128), F32),
        ((32, 128), F32), ((2, 8, 4, 128), F32), ((2, 8, 4, 128), BF16), ((2, 32, 4, 128), BF16), ((2, 128, 128), F32), ((2, 64, 384), F32),
        ((2, 32, 2, 384), F32), ((2, 32, 2, 384), F32),
        ((2, 2, 128), F32), ((2, 16, 128), F32), ((2, 4, 128), F32), ((2, 2, 256), F32),
        ((2, 16, 128), F32), ((2, 16, 128), BF16), ((16, 2, 16, 128), BF16), ((512, 128), F32),
        ((32, 128), BF16), ((16, 4, 32, 128), BF16), ((2, 1024, 128), F32),
        ((SLOTS - OWN, D), F32), ((2, 2, SLOTS, 512), F32),
        ((8, 2 * SLOTS, 256), BF16), ((CHIPS, 16, 256), BF16), ((CHIPS, 16, 256), BF16), ((2, D), F32),
    ]
    packed = pl.pallas_call(
        kernel,
        out_shape=jax.ShapeDtypeStruct((2, D + 1024), BF16),
        in_specs=[hbm] * 20,
        out_specs=pl.BlockSpec(memory_space=pltpu.VMEM),
        scratch_shapes=[pltpu.SMEM((2,), jnp.int32)]
        + [pltpu.VMEM(*s) for s in scratch]
        + [pltpu.SemaphoreType.DMA((20,)), pltpu.SemaphoreType.DMA((15,)), pltpu.SemaphoreType.DMA((15,))]
        + [pltpu.SemaphoreType.REGULAR],
        compiler_params=pltpu.CompilerParams(
            collective_id=0, has_side_effects=True, vmem_limit_bytes=60 * 1024 * 1024
        ),
    )(
        lengths, hidden_in, lam_heads.reshape(1, 8), head_gain.reshape(1, 256),
        attn_gain.reshape(1, D), moe_gain.reshape(1, D), routing.T, route_weight.T,
        query_w, key_w, value_w, out_w, key_cache, value_cache, gate_w, up_w, down_w,
        shared_gate, shared_up, shared_down,
    )

    def unpack(src, layer, key, value):
        layer[...] = src[:, 0:D]
        key[...] = src[:, D : D + 512]
        value[...] = src[:, D + 512 :]

    vmem = pl.BlockSpec(memory_space=pltpu.VMEM)
    return pl.pallas_call(
        unpack,
        out_shape=(
            jax.ShapeDtypeStruct((2, D), BF16),
            jax.ShapeDtypeStruct((2, 512), BF16),
            jax.ShapeDtypeStruct((2, 512), BF16),
        ),
        in_specs=[vmem],
        out_specs=(vmem, vmem, vmem),
        compiler_params=pltpu.CompilerParams(vmem_limit_bytes=60 * 1024 * 1024),
    )(packed)


def solution(mesh):
    e2, e3 = P("ep", None), P("ep", None, None)
    return jax.shard_map(
        on_device,
        mesh=mesh,
        in_specs=(
            e2, P("ep"), e3, e3, e2, e2, e2, e2, P(), P(), P(), P(), P(), P(), e3, e3, e3, P(), P(), P(),
        ),
        out_specs=(e2, e2, e2),
        check_vma=False,
    )
```

```python
import jax
import jax.numpy as jnp
from jax import lax
from jax.experimental import pallas as pl
from jax.experimental.pallas import tpu as pltpu
from jax.sharding import PartitionSpec as P

F32 = jnp.float32
BF16 = jnp.bfloat16
MESH = pl.DeviceIdType.MESH
N = 128
CHIPS = 64
D = 2048
CACHE = 1024
SLOTS = 32
OWN = 24
W, O, OX, HID, P1, P2, P3, GX, UX, DX, P6, P5 = range(12)


def dot(a, b):
    return jnp.dot(a, b, preferred_element_type=F32)


def dot_nt(a, b):
    return lax.dot_general(a, b, (((1,), (1,)), ((), ())), preferred_element_type=F32)


def rem(a, b):
    return lax.rem(a, jnp.int32(b))


def div(a, b):
    return lax.div(a, jnp.int32(b))


def kind(v):
    return rem(div(v + 1, 2), 2)


def far(pair):
    return -sum(min(k, 4 - k) for k in pair)


NEAR = sorted(((a, b) for a in range(4) for b in range(4)), key=far)
ALL = sorted(((a, b, k) for a in range(4) for b in range(4) for k in range(4)), key=far)[:-1]


def iota(shape, dim):
    return lax.broadcasted_iota(jnp.int32, shape, dim)


def rms(x, gain, eps):
    return x * lax.rsqrt(jnp.mean(x * x, axis=-1, keepdims=True) + eps) * gain


def kernel(
    lengths_h, hidden_h, lam_h, hgain_h, again_h, mgain_h, routing_h, rweight_h,
    qw, kw, vw, ow, kc_h, vc_h, gate_h, up_h, down_h, sg_h, su_h, sd_h,
    out,
    lengths, hidden, lam, hgain, again, mgain, routing, rweight,
    wcat, obuf_s, wbuf, obuf, kc, vc, gate, up, down, gate_x, up_x, down_x, sg, su, sd,
    hs, hbuf, hb, lines, s1f, s1, r1, x1, part, s2, r2, angles, qscr, kscr, vscr, at16, s3, r3, x3,
    am, gat, spread, mine, pre, ans, res, racc, fin,
    loc, snd, rcv, met,
):
    me = lax.axis_index("ep")
    z = div(me, 32)
    y = rem(div(me, 8), 4)
    xc = rem(me, 8)
    c = rem(me, 2)
    chip = div(me, 2)
    q = rem(chip, 16)
    mate = me + 1 - 2 * c

    x = div(xc, 2)
    z_at = [rem(z + k, 4) for k in range(4)]
    y_at = [rem(y + k, 4) for k in range(4)]
    x_at = [rem(x + k, 4) for k in range(4)]
    flips = sorted(((a, b, k, e) for a in (0, 1) for b in (0, 1) for k in (0, 1) for e in (0, 1)), key=sum)[:0:-1]
    hops = sorted(
        ((a, b, k, e) for a in range(4) for b in (0, 1) for k in (0, 1) for e in (0, 1)),
        key=lambda h: -(min(h[0], 4 - h[0]) + h[1] + h[2] + 0.1 * h[3]),
    )[:-1]
    cube_peers, cube_row, cube_col, group_peers, seat, my_kind = [], [], [], [], [], []
    for h in range(2):
        zs, ys, xs = (rem(v + h, 4) for v in (z, y, x))
        zo, yo, xo = (rem(7 - v - h, 4) for v in (zs, ys, xs))
        long, pair = (zs, xs) if h == 0 else (xs, zs)
        peers = []
        for a, b, k, e in flips:
            zt, yt, xt, ct = (z, zo)[a], (y, yo)[b], (x, xo)[k], (c, 1 - c)[e]
            lt = rem((zt, xt)[h] + h, 4)
            col = pl.multiple_of(h * 1536 + (div(lt, 2) * 2 + ct) * 384, 128)
            peers.append((zt * 32 + yt * 8 + xt * 2 + ct, col))
        cube_peers.append(peers)
        at = div(zs, 2) * 128 + div(ys, 2) * 64 + c * 16
        cube_row.append(pl.multiple_of(at + 32 * jnp.where(kind(xs) == 1, div(xs, 2), 1 - div(xs, 2)), 16))
        cube_col.append(pl.multiple_of(h * 1536 + (div(long, 2) * 2 + c) * 384, 128))
        seat.append(((long * 2 + rem(ys, 2)) * 2 + rem(pair, 2)) * 2 + c)
        my_kind.append((kind(zs) * 2 + kind(ys)) * 2 + kind(xs))
        peers = []
        for a, b, k, e in hops:
            lt, ct = rem(long + a, 4), (c, 1 - c)[e]
            yt, pt = (ys, ys + 1 - 2 * rem(ys, 2))[b], (pair, pair + 1 - 2 * rem(pair, 2))[k]
            there = ((lt * 2 + rem(yt, 2)) * 2 + rem(pt, 2)) * 2 + ct
            zt, xt = (lt, pt) if h == 0 else (pt, lt)
            which = (kind(zt) * 2 + kind(yt)) * 2 + kind(xt)
            device = rem(zt + 4 - h, 4) * 32 + rem(yt + 4 - h, 4) * 8 + rem(xt + 4 - h, 4) * 2 + ct
            peers.append((device, there, which))
        group_peers.append(peers)
    chips = [z_at[dz] * 16 + y_at[dy] * 4 + x_at[dx] for dz, dy, dx in ALL]

    barrier = pltpu.get_barrier_semaphore()

    def greet(semaphore, device):
        pl.semaphore_signal(semaphore, inc=1, device_id=(device,), device_id_type=MESH)

    pairs = [
        (hidden_h, hidden), (again_h, again),
        (qw, wcat.at[:, pl.ds(0, 2048)]), (kw, wcat.at[:, pl.ds(2048, 512)]), (vw, wcat.at[:, pl.ds(2560, 512)]),
        (routing_h, routing), (rweight_h, rweight), (ow, obuf_s),
        (kc_h, kc), (vc_h, vc), (lengths_h, lengths), (lam_h, lam), (hgain_h, hgain), (mgain_h, mgain),
        (gate_h.at[0], gate), (up_h.at[0], up), (down_h.at[0], down), (sg_h, sg), (su_h, su), (sd_h, sd),
    ]
    copies = [pltpu.make_async_copy(src, dst, loc.at[i]) for i, (src, dst) in enumerate(pairs)]
    for copy in copies[:5]:
        copy.start()

    for i, (a, b, k, e) in enumerate(hops):
        greet(barrier, group_peers[0][i][0])
        if b:
            greet(barrier, group_peers[1][i][0])
    for zt in (z, 3 - z):
        for xt in (3 - x, 3 - (x + 1 - 2 * rem(x, 2))):
            for ct in (c, 1 - c):
                greet(barrier, zt * 32 + y * 8 + xt * 2 + ct)
    for copy in copies[5:]:
        copy.start()

    def ready(lo, hi):
        for copy in copies[lo:hi]:
            copy.wait()

    def remote(src, dst, phase, device):
        return pltpu.make_async_remote_copy(
            src_ref=src, dst_ref=dst, send_sem=snd.at[phase], recv_sem=rcv.at[phase],
            device_id=(device,), device_id_type=MESH,
        )

    def arrived(ref, phase):
        remote(ref, ref, phase, mate).wait_recv()

    def left(ref, phase):
        remote(ref, ref, phase, mate).wait_send()

    ready(0, 2)
    h32 = hidden[...].astype(F32)
    normed = rms(h32, again[...], 1e-6).astype(BF16).astype(F32)
    for i in range(2):
        for b in range(16):
            lines[i * 16 + b : i * 16 + b + 1, :] = normed[i : i + 1, b * 128 : b * 128 + 128]
    low = iota((1, 128), 1) < 64
    turned = [pltpu.roll(lines[...], 32 * i, 1) for i in (1, 2, 3)] + [lines[...]]
    for h in range(2):
        for which in range(8):
            sz, sy, sx = which // 4, which // 2 % 2, which % 2
            first_half, second_half = turned[h + 2 * sx], turned[(h + 2 - 2 * sx) % 4]
            for i in range(2):
                for zi in range(2):
                    zz = (((0, 3), (1, 2))[sz][zi] - h) % 4
                    left_at, right_at = (i * 16 + zz * 4 + (yy - h) % 4 for yy in ((0, 3), (1, 2))[sy])
                    line = jnp.where(low, first_half[left_at : left_at + 1], second_half[right_at : right_at + 1])
                    s1f[h, which, i * 2 + zi : i * 2 + zi + 1, :] = line
    s1[...] = s1f[...].astype(BF16)
    for j in range(16):
        hs[j] = h32[:, j * 128 : j * 128 + 128]
    ready(2, 5)
    pl.semaphore_wait(barrier, 55)

    for h in range(2):
        for device, there, which in group_peers[h]:
            remote(s1.at[h, which], r1.at[h, seat[h]], P1, device).start()
    for i in range(15):
        for h in range(2):
            device, col = cube_peers[h][i]
            remote(
                wcat.at[:, pl.ds(col, 384)], wbuf.at[h, pl.ds(cube_row[h], 16), :], W, device
            ).start()
    for device, there, which in group_peers[0]:
        greet(met, device)
    for h in range(2):
        wbuf[h, pl.ds(cube_row[h], 16), :] = wcat[:, pl.ds(cube_col[h], 384)]
        r1[h, seat[h]] = s1[h, my_kind[h]]
    hbuf[q] = hs[q]

    ready(5, 8)
    obuf[chip, c] = obuf_s[:, pl.ds(pl.multiple_of(q * 128, 128), 128)]
    sel = jnp.where(
        iota((128, 256), 1) == 4 * (iota((128, 256), 0) // 2) + 2 * c + iota((128, 256), 0) % 2, 1.0, 0.0
    ).astype(BF16)
    before = jnp.where(iota((256, 256), 0) < iota((256, 256), 1), 1.0, 0.0).astype(BF16)
    picks, back, slot_weight = [], [], []
    for i, expert in enumerate((me, mate)):
        hit = routing[...] == expert
        here = jnp.sum(jnp.where(hit, 1.0, 0.0), axis=0, keepdims=True)
        rank = dot(jnp.broadcast_to(here, (16, 256)).astype(BF16), before)[0:1]
        full = jnp.where(rank == iota((SLOTS, 256), 0).astype(F32), here, 0.0)
        back.append(dot_nt(sel, full.astype(BF16)))
        weight = jnp.sum(jnp.where(hit, rweight[...], 0.0), axis=0, keepdims=True)
        slot_weight.append(jnp.sum(full * weight, axis=1, keepdims=True))
        mark = (iota((SLOTS, 256), 0) - OWN == iota((SLOTS, 256), 1) - 2 * expert) & (
            iota((SLOTS, 256), 1) // 2 == expert
        )
        full = full + jnp.where(mark, 1.0, 0.0)
        picks.append(dot_nt(full.astype(BF16), sel))
    picks = jnp.concatenate(picks, axis=0).astype(BF16)
    back = jnp.concatenate(back, axis=1).astype(BF16)

    ready(14, 17)
    remote(gate, gate_x, GX, mate).start()
    remote(up, up_x, UX, mate).start()
    ready(8, 14)
    lane = iota((1, 128), 1)
    inverse = jnp.exp((lane % 64).astype(F32) * (-13.122363377404328 / 64))
    for s in range(2):
        angle = lengths[s].astype(F32) * inverse
        angles[0, s : s + 1, :] = jnp.cos(angle)
        angles[1, s : s + 1, :] = jnp.where(lane < 64, -jnp.sin(angle), jnp.sin(angle))

    arrived(r1.at[:, pl.ds(0, 31)], P1)
    for h in range(2):
        for i in range(32):
            x1[h, 4 * i : 4 * i + 4, :] = r1[h, i].astype(F32)
    arrived(wbuf.at[:, pl.ds(0, 240), :], W)
    for h in range(2):
        wide = jnp.concatenate([x1[h, pl.ds(b, 64, stride=2), :].astype(BF16) for b in range(2)], axis=1)
        part[h] = dot(wide, wbuf[h])
        for i in range(32):
            s2[h, i] = part[h, 2 * i : 2 * i + 2, :]

    for i in range(31):
        for h in range(2):
            device, there, which = group_peers[h][i]
            remote(s2.at[h, there], r2.at[h, seat[h]], P2, device).start()
    for h in range(2):
        r2[h, seat[h]] = s2[h, seat[h]]
    pl.semaphore_wait(met, 31)
    for t in chips:
        col = pl.multiple_of(rem(t, 16) * 128, 128)
        remote(obuf_s.at[:, pl.ds(col, 128)], obuf.at[chip, c], O, t * 2 + c).start()
    for dy, dx in NEAR[:-1]:
        t = y_at[dy] * 4 + x_at[dx]
        remote(hs.at[t], hbuf.at[q], HID, z * 32 + t * 2 + c).start()
    remote(down, down_x, DX, mate).start()
    arrived(r2.at[:, pl.ds(0, 31)], P2)

    for u in range(24):
        at = (u % 3) * 128
        val = None
        for src in range(32):
            if (src // 16) * 2 + src % 2 == u // 3 % 4:
                term = r2[u // 12, src, :, at : at + 128]
                val = term if val is None else val + term
        for s in range(2):
            line = val[s : s + 1, :]
            if u < 16:
                r = (u % 2) * 8 + u // 2
                qscr[s, r : r + 1, :] = line
            elif u < 20:
                kscr[s, u - 16 : u - 15, :] = line
            else:
                v = u - 20
                vscr[s, v // 2 : v // 2 + 1, (v % 2) * 128 : (v % 2) * 128 + 128] = line

    rows = iota((16, 1), 0)
    pair_of = (rows // 8) + 2 * ((rows % 8) // 4)
    first = iota((8, 1), 0) < 4
    lam_col = jnp.sum(jnp.where(iota((8, 8), 0) == iota((8, 8), 1), lam[...], 0.0), axis=1, keepdims=True)
    scale = 128 ** (-0.5)

    def turn(v, cos_row, sin_row):
        return (v * cos_row + pltpu.roll(v, 64, 1) * sin_row).astype(BF16)

    q_rows, k_rows, v_rows, all_scores = [], [], [], []
    for s in range(2):
        cos_row, sin_row = angles[0, s : s + 1, :], angles[1, s : s + 1, :]
        qq = turn(qscr[s], cos_row, sin_row).astype(F32)
        wide = jnp.concatenate([jnp.where(pair_of == u, qq, 0.0) for u in range(4)], axis=1).astype(BF16)
        all_scores.append(dot_nt(wide, kc[s]))
        kn = turn(kscr[s], cos_row, sin_row)
        vn = vscr[s].astype(BF16)
        for u in range(4):
            out[s : s + 1, D + u * 128 : D + u * 128 + 128] = kn[u : u + 1]
        for u in range(2):
            out[s : s + 1, D + 512 + u * 256 : D + 512 + u * 256 + 256] = vn[u : u + 1]
        q_rows.append(qq)
        k_rows.append(kn.astype(F32))
        v_rows.append(vn.astype(F32))
    sums, own_parts = [], []
    for s in range(2):
        qq, kn = q_rows[s], k_rows[s]
        scores = all_scores[s] * scale
        k_of = jnp.where(
            pair_of == 0, kn[0:1], jnp.where(pair_of == 1, kn[1:2], jnp.where(pair_of == 2, kn[2:3], kn[3:4]))
        )
        own_score = jnp.sum(qq * k_of, axis=1, keepdims=True) * scale
        live = iota((1, CACHE), 1) < lengths[s]
        peak = jnp.maximum(jnp.max(jnp.where(live, scores, -jnp.inf), axis=1, keepdims=True), own_score)
        weights = jnp.where(live, jnp.exp(scores - peak), 0.0)
        own_weight = jnp.exp(own_score - peak)
        share = 1.0 / (jnp.sum(weights, axis=1, keepdims=True) + own_weight)
        maps = weights * share
        own_maps = own_weight * share
        combined = (maps[:8] - lam_col * maps[8:]).astype(BF16)
        own_parts.append((own_maps[:8] - lam_col * own_maps[8:]).astype(BF16).astype(F32))
        sums.append(dot(combined, vc[s]))
    for s in range(2):
        head_out = jnp.where(first, sums[s][:, :256], sums[s][:, 256:])
        head_out = head_out + own_parts[s] * jnp.where(first, v_rows[s][0:1], v_rows[s][1:2])
        att = rms(head_out, hgain[...], 1e-5)
        for h in range(8):
            for half in range(2):
                at16[s, 2 * h + half : 2 * h + half + 1, :] = att[h : h + 1, half * 128 : half * 128 + 128]
        s3[s] = at16[s].astype(BF16)

    for dy, dx in NEAR[:-1]:
        t = y_at[dy] * 4 + x_at[dx]
        remote(s3, r3.at[q], P3, z * 32 + t * 2 + c).start()
    r3[q] = s3[...]
    arrived(obuf.at[pl.ds(0, 63), 0], O)
    remote(obuf.at[:, c], obuf.at[:, c], OX, mate).start()
    arrived(hbuf.at[pl.ds(0, 15)], HID)
    for i in range(16):
        hb[2 * i : 2 * i + 2, :] = hbuf[i]
    arrived(obuf.at[:, 0], OX)
    arrived(r3.at[pl.ds(0, 15)], P3)
    x3[...] = r3[...].reshape(512, 128).astype(F32)
    wide = jnp.concatenate([x3[pl.ds(b, 32, stride=16), :].astype(BF16) for b in range(16)], axis=1)
    proj = dot(wide, obuf[...].reshape(D, 128))
    mixed = (hb[...] + proj.astype(BF16).astype(F32)).astype(BF16)
    am[...] = mixed
    gat[q, z] = mixed

    for dy in (2, 1, 3, 0):
        for dz, dx in NEAR if dy else NEAR[:-1]:
            t = z_at[dz] * 16 + y_at[dy] * 4 + x_at[dx]
            remote(am, gat.at[q, z], P5 + dy, t * 2 + c).start()
    ready(17, 20)
    squares = jnp.zeros((2 * SLOTS, 1), F32)
    for k, dy in enumerate((2, 1, 3, 0)):
        arrived(racc.at[pl.ds(0, 16 if dy else 15)], P5 + dy)
        if k == 0:
            arrived(gate_x, GX)
            arrived(up_x, UX)
            arrived(down_x, DX)
        ys = y_at[4 - dy if dy else 0]
        at = pl.multiple_of(ys * 512, 512)
        tiles = [gat[ys * 4 + i].reshape(128, 128) for i in range(4)]
        got = jnp.concatenate(
            [dot(picks, jnp.concatenate(tiles[i : i + 2], axis=1)) for i in (0, 2)], axis=1
        )
        mine[:, pl.ds(at, 512)] = got[OWN:SLOTS]
        squares = squares + jnp.sum(got * got, axis=1, keepdims=True)
        got = (got * mgain[:, pl.ds(at, 512)]).astype(BF16)
        for i, (g, u) in enumerate(((gate, up), (gate_x, up_x))):
            rows = got[i * SLOTS : i * SLOTS + SLOTS]
            for j, w in enumerate((g, u)):
                term = dot(rows, w[pl.ds(at, 512), :])
                pre[i, j] = term if k == 0 else pre[i, j] + term
    factor = lax.rsqrt(squares / D + 1e-6)
    for i, d in enumerate((down, down_x)):
        f = factor[i * SLOTS : i * SLOTS + SLOTS]
        hid = (jax.nn.silu(pre[i, 0] * f) * (pre[i, 1] * f)).astype(BF16)
        answer = dot(hid, d[...]).astype(BF16).astype(F32) * slot_weight[i]
        for b in range(8):
            ans[b, i * SLOTS : i * SLOTS + SLOTS] = answer[:, b * 256 : b * 256 + 256].astype(BF16)
    for b in range(8):
        tiles = dot(back, ans[b])
        for half in range(2):
            spread[half, pl.ds(b, 128, stride=8), :] = tiles[:, half * 128 : half * 128 + 128]
    for k in (2, 1, 3, 0):
        owners = pl.ds(pl.multiple_of(z_at[k] * 16, 16), 16)
        rows = pl.ds(pl.multiple_of(z_at[k] * 256, 256), 256)
        tiles = jnp.concatenate([spread[0, rows, :], spread[1, rows, :]], axis=1)
        res[owners] = tiles.astype(BF16).reshape(16, 16, 256)
        for dy, dx in NEAR if k else NEAR[:-1]:
            t = z_at[k] * 16 + y_at[dy] * 4 + x_at[dx]
            remote(res.at[t], racc.at[chip], P6, t * 2 + c).start()
    racc[chip] = res[chip]
    mixed = mine[...]
    moe = rms(mixed, mgain[...], 1e-6).astype(BF16)
    hid = (jax.nn.silu(dot(moe, sg[...])) * dot(moe, su[...])).astype(BF16)
    shared = dot(hid, sd[...])
    left(wbuf.at[:, pl.ds(0, 240), :], W)
    left(obuf.at[pl.ds(0, 63), 0], O)
    left(obuf.at[:, 0], OX)
    left(hbuf.at[pl.ds(0, 15)], HID)
    left(r1.at[:, pl.ds(0, 31)], P1)
    left(r2.at[:, pl.ds(0, 31)], P2)
    left(r3.at[pl.ds(0, 15)], P3)
    for dy in range(4):
        left(racc.at[pl.ds(0, 16 if dy else 15)], P5 + dy)
    left(gate, GX)
    left(up, UX)
    left(down, DX)
    arrived(racc.at[pl.ds(0, CHIPS - 1)], P6)

    def add(i, carry):
        return carry + racc[i].astype(F32)

    total = lax.fori_loop(0, CHIPS, add, jnp.zeros((16, 256), F32), unroll=8)
    for s in range(2):
        for b in range(8):
            fin[s : s + 1, b * 256 : b * 256 + 256] = total[s * 8 + b : s * 8 + b + 1]
    out[:, 0:D] = (mixed[0:2] + fin[...] + shared[0:2]).astype(BF16)
    left(racc.at[pl.ds(0, CHIPS - 1)], P6)


def on_device(
    hidden_in, lengths, key_cache, value_cache, query_w, key_w, value_w, out_w, lam_heads, head_gain,
    attn_gain, moe_gain, routing, route_weight, gate_w, up_w, down_w, shared_gate, shared_up, shared_down,
):
    hbm = pl.BlockSpec(memory_space=pl.ANY)
    scratch = [
        ((2, D), BF16), ((1, 8), F32), ((1, 256), F32), ((1, D), F32), ((1, D), F32),
        ((6, 256), jnp.int32), ((6, 256), F32),
        ((16, 3072), BF16), ((16, D), BF16), ((2, 256, 384), BF16), ((CHIPS, 2, 16, 128), BF16),
        ((2, CACHE, 512), BF16), ((2, CACHE, 512), BF16),
        ((D, 512), BF16), ((D, 512), BF16), ((512, D), BF16),
        ((D, 512), BF16), ((D, 512), BF16), ((512, D), BF16),
        ((D, 512), BF16), ((D, 512), BF16), ((512, D), BF16),
        ((16, 2, 128), F32), ((16, 2, 128), F32), ((32, 128), F32),
        ((32, 128), F32), ((2, 8, 4, 128), F32), ((2, 8, 4, 128), BF16), ((2, 32, 4, 128), BF16), ((2, 128, 128), F32), ((2, 64, 384), F32),
        ((2, 32, 2, 384), F32), ((2, 32, 2, 384), F32),
        ((2, 2, 128), F32), ((2, 16, 128), F32), ((2, 4, 128), F32), ((2, 2, 256), F32),
        ((2, 16, 128), F32), ((2, 16, 128), BF16), ((16, 2, 16, 128), BF16), ((512, 128), F32),
        ((32, 128), BF16), ((16, 4, 32, 128), BF16), ((2, 1024, 128), F32),
        ((SLOTS - OWN, D), F32), ((2, 2, SLOTS, 512), F32),
        ((8, 2 * SLOTS, 256), BF16), ((CHIPS, 16, 256), BF16), ((CHIPS, 16, 256), BF16), ((2, D), F32),
    ]
    packed = pl.pallas_call(
        kernel,
        out_shape=jax.ShapeDtypeStruct((2, D + 1024), BF16),
        in_specs=[hbm] * 20,
        out_specs=pl.BlockSpec(memory_space=pltpu.VMEM),
        scratch_shapes=[pltpu.SMEM((2,), jnp.int32)]
        + [pltpu.VMEM(*s) for s in scratch]
        + [pltpu.SemaphoreType.DMA((20,)), pltpu.SemaphoreType.DMA((15,)), pltpu.SemaphoreType.DMA((15,))]
        + [pltpu.SemaphoreType.REGULAR],
        compiler_params=pltpu.CompilerParams(
            collective_id=0, has_side_effects=True, vmem_limit_bytes=60 * 1024 * 1024
        ),
    )(
        lengths, hidden_in, lam_heads.reshape(1, 8), head_gain.reshape(1, 256),
        attn_gain.reshape(1, D), moe_gain.reshape(1, D), routing.T, route_weight.T,
        query_w, key_w, value_w, out_w, key_cache, value_cache, gate_w, up_w, down_w,
        shared_gate, shared_up, shared_down,
    )

    def unpack(src, layer, key, value):
        layer[...] = src[:, 0:D]
        key[...] = src[:, D : D + 512]
        value[...] = src[:, D + 512 :]

    vmem = pl.BlockSpec(memory_space=pltpu.VMEM)
    return pl.pallas_call(
        unpack,
        out_shape=(
            jax.ShapeDtypeStruct((2, D), BF16),
            jax.ShapeDtypeStruct((2, 512), BF16),
            jax.ShapeDtypeStruct((2, 512), BF16),
        ),
        in_specs=[vmem],
        out_specs=(vmem, vmem, vmem),
        compiler_params=pltpu.CompilerParams(vmem_limit_bytes=60 * 1024 * 1024),
    )(packed)


def solution(mesh):
    e2, e3 = P("ep", None), P("ep", None, None)
    return jax.shard_map(
        on_device,
        mesh=mesh,
        in_specs=(
            e2, P("ep"), e3, e3, e2, e2, e2, e2, P(), P(), P(), P(), P(), P(), e3, e3, e3, P(), P(), P(),
        ),
        out_specs=(e2, e2, e2),
        check_vma=False,
    )
```
